512 devices in a mesh: ep: 128 (over z, x, core), tp: 4 (over y).
Axes of the slice: x: 4, y: 4, z: 16, core: 2. Of those that a mesh axis runs over, the one named last changes fastest.
Arguments:
- tokens: bfloat16 [16384, 2048], P('ep'), may hold values from -6 to 6
- pre_gain: float32 [2048], replicated, may hold values from 0.1 to 1.9
- post_gain: float32 [2048], P('tp'), may hold values from 0.1 to 1.9
- expert_ids: int32 [16384, 2], P('ep'), may hold values from 0 to 127, all different within a row; in each aligned block of 128 rows (0 to 127, 128 to 255, ...) at most 3 rows name the same one
- route_weights: float32 [16384, 2], P('ep'), may hold values from 0.1 to 1
- w_gate: bfloat16 [128, 2048, 512], P('ep', None, 'tp'), may hold values from -0.125 to 0.125
- w_up: bfloat16 [128, 2048, 512], P('ep', None, 'tp'), may hold values from -0.125 to 0.125
- w_down: bfloat16 [128, 512, 2048], P('ep', None, 'tp'), may hold values from -0.25 to 0.25
Outputs:
- routed: bfloat16 [16384, 2048], P('ep', 'tp')
The draws below stay inside these ranges and needn't reach their ends.
Inputs may be any that keep to these rules, and one draw needn't show every extreme that they name: `expert_ids`: each row names 2 different experts. Among the rows of one index of ep (aligned blocks of 128 rows) no expert is named by more than 3 rows, a bound that some block reaches.
All inputs are finite; a program needn't handle non-finite values.
Results may differ from the reference program's by a relative error of at most 0.007.
Values may be sent and summed in bfloat16 or wider, within the bound.
No kernel may reach another device: no remote copies, remote signals or barrier semaphores. Data moves between devices by JAX's collectives and lax.ppermute only.
A program may use at most 64 MiB of HBM per device.

```python
import math
import jax
import jax.numpy as jnp
import numpy as np
from jax import lax

D = 2048
FF = 512
TOP = 2
TOK_EP = 128
EXPERTS = 128
CAP = 3
TOKENS = 16384
N_EP = 128


def levels(own_key, shape, shards, least, high):
    def one(dim, blocks):
        draws = jax.random.uniform(jax.random.fold_in(jax.random.fold_in(own_key, 6), dim), (blocks,), jnp.float32, least / len(shards), high / len(shards))
        return jnp.repeat(jnp.exp(draws), shape[dim] // blocks).reshape((-1,) + (1,) * (len(shape) - dim - 1))

    loudness = one(*shards[0])
    for cut in shards[1:]:
        loudness = loudness * one(*cut)
    return loudness


def routed_block(rng, own, number, rows, count, top, limit, slope):
    order = jax.random.permutation(rng, count)
    heavy_load, ordinary = portions_of(count, rows * top, limit, slope, True), portions_of(count, rows * top, limit, slope, False)
    places = jnp.arange(count)

    def named(tallies, offset_by):
        used = int((tallies > 0).sum())
        fixed = max(1, used // 4)
        shifted = fixed + (places - fixed + offset_by * (used - fixed)) % max(1, count - fixed)
        return jnp.zeros((count,), jnp.int32).at[order[jnp.where(places < fixed, places, shifted)]].set(jnp.asarray(tallies, jnp.int32))

    tallies = jnp.where(number % 4 == 0, named(heavy_load, number // 4), named(ordinary, number - number // 4 - 1))
    mixed = jax.random.permutation(jax.random.fold_in(own, 3), count)
    giver, receiver = mixed[0:count // 2 * 2:2], mixed[1:count // 2 * 2:2]
    room = jnp.minimum(tallies[giver] - 1, limit - tallies[receiver]) // 2
    room = jnp.where((giver == order[0]) | (receiver == order[0]) | (tallies[receiver] == 0), 0, jnp.maximum(room, 0))
    shifted = jax.random.randint(jax.random.fold_in(own, 4), (count // 2,), 0, 1 << 20) % (room + 1)
    tallies = tallies.at[giver].add(-shifted).at[receiver].add(shifted)
    labels = jnp.searchsorted(jnp.cumsum(tallies), jnp.arange(rows * top), side="right").astype(jnp.int32)
    table = labels.reshape(top, rows).T
    table = table[jax.random.permutation(jax.random.fold_in(own, 1), rows)]
    offset_by = jax.random.randint(jax.random.fold_in(own, 2), (rows, 1), 0, top)
    return jnp.take_along_axis(table, (jnp.arange(top)[None, :] + offset_by) % top, axis=1)


def portions_of(amount, total, reach, lean, full):
    loads = [(1 << 20) // math.isqrt(standing ** lean) + 1 for standing in range(1, amount + 1)]
    largest = reach if full else min(reach, max(-(-total // amount), total * loads[0] // sum(loads)))
    least = 1 if total - largest >= amount - 1 else 0
    counts, spare = [largest] + [least] * (amount - 1), total - largest - least * (amount - 1)
    while spare > 0:
        movable = [i for i in range(1, amount) if counts[i] < largest] or [i for i in range(1, amount) if counts[i] < reach]
        mass, left = sum([loads[i] for i in movable]), spare
        for i in movable:
            more = min(reach - counts[i], max(1, left * loads[i] // mass), spare)
            counts[i] = counts[i] + more
            spare = spare - more
    return np.array(counts)


def centred(key, dims, spread, bound, cuts=(), kind=jnp.bfloat16):
    loudness = levels(key, dims, cuts, -0.22, 0.18) if cuts else 1.0
    drawn = jax.random.normal(key, dims, jnp.float32) * spread * loudness
    return jnp.minimum(jnp.maximum(drawn, -bound), bound).astype(kind)


def setup_inputs(seed: int = 0) -> dict:
    key_of = jax.random.split(jax.random.key(seed), 9)
    tokens = centred(key_of[0], (TOKENS, D), 1.0, 6.0, ((0, 128),))
    pre_gain = jnp.clip(1.0 + 0.18 * jax.random.normal(key_of[1], (D,), jnp.float32), 0.1, 1.9)
    post_gain = jnp.clip(1.0 + 0.18 * jax.random.normal(key_of[2], (D,), jnp.float32), 0.1, 1.9)
    expert_ids_keys = jax.random.split(jax.random.fold_in(key_of[3], 1), TOKENS // TOK_EP)
    expert_ids_turns = jax.random.permutation(jax.random.fold_in(key_of[3], 3), TOKENS // TOK_EP)
    expert_ids = jax.vmap(lambda own, number: routed_block(jax.random.fold_in(key_of[3], 2), own, number, TOK_EP, EXPERTS, TOP, CAP, 2))(expert_ids_keys, expert_ids_turns).reshape((TOKENS, TOP))
    route_weights = jnp.clip(0.1 + 0.9 * jax.random.uniform(key_of[4], (TOKENS, TOP), jnp.float32) ** levels(key_of[4], (TOKENS, TOP), ((0, 128),), -0.2, 0.2), 0.1, 1.0)
    w_gate = centred(key_of[5], (EXPERTS, D, FF), D ** -0.5, 0.125, ((0, 128), (2, 4)))
    w_up = centred(key_of[6], (EXPERTS, D, FF), D ** -0.5, 0.125, ((0, 128), (2, 4)))
    w_down = centred(key_of[7], (EXPERTS, FF, D), FF ** -0.5, 0.25, ((0, 128), (2, 4)))
    return dict(tokens=tokens, pre_gain=pre_gain, post_gain=post_gain, expert_ids=expert_ids, route_weights=route_weights, w_gate=w_gate, w_up=w_up, w_down=w_down)


epsilon = 1e-06

def reference(tokens, pre_gain, post_gain, expert_ids, route_weights, w_gate, w_up, w_down):
    total_rows, row_width = tokens.shape
    values = tokens.astype(jnp.float32)
    row_scale = lax.rsqrt(lax.optimization_barrier(jnp.mean(values * values, axis=1, keepdims=True)) + epsilon)
    normed = (values * row_scale * pre_gain[None, :]).astype(jnp.bfloat16)
    expert_count = w_gate.shape[0]
    pick_count = expert_ids.shape[1]
    block_count = N_EP
    block_rows = total_rows // block_count
    pick_total = block_rows * pick_count
    flat_ids = expert_ids.reshape(block_count, pick_total).astype(jnp.int32)
    onehot = (flat_ids[:, :, None] == jnp.arange(expert_count, dtype=jnp.int32)[None, None, :]).astype(jnp.int32)
    earlier = jnp.cumsum(onehot, axis=1) - onehot
    slot_index = lax.optimization_barrier(jnp.sum(earlier * onehot, axis=2)).astype(jnp.int32)
    block_index = jnp.broadcast_to(jnp.arange(block_count, dtype=jnp.int32)[:, None], (block_count, pick_total))
    token_index = block_index * block_rows + (jnp.arange(pick_total, dtype=jnp.int32) // pick_count)[None, :]
    owners = jnp.full((expert_count, block_count, CAP), -1, jnp.int32).at[flat_ids, block_index, slot_index].set(token_index)
    weight_of = jnp.zeros((expert_count, block_count, CAP), jnp.float32).at[flat_ids, block_index, slot_index].set(route_weights.reshape(block_count, pick_total))

    def one_expert(mixed, items):
        owner_rows, weights, gate_w, up_w, down_w = items
        owner_rows = owner_rows.reshape(-1)
        live = owner_rows >= 0
        safe_rows = jnp.where(live, owner_rows, 0)
        gathered = normed[safe_rows]
        gate_sum = jnp.dot(gathered, gate_w, preferred_element_type=jnp.float32)
        up_sum = jnp.dot(gathered, up_w, preferred_element_type=jnp.float32)
        hidden = (jax.nn.silu(gate_sum) * up_sum).astype(jnp.bfloat16)
        expert_out = jnp.dot(hidden, down_w, preferred_element_type=jnp.float32).astype(jnp.bfloat16)
        expert_out = lax.optimization_barrier(expert_out).astype(jnp.float32)
        added = jnp.where(live[:, None], expert_out * weights.reshape(-1)[:, None], 0.0)
        return (mixed.at[safe_rows].add(added), None)
    start = jnp.zeros((total_rows, row_width), jnp.float32)
    mixed, _ = lax.scan(one_expert, start, (owners, weight_of, w_gate, w_up, w_down))
    out_scale = lax.rsqrt(lax.optimization_barrier(jnp.mean(mixed * mixed, axis=1, keepdims=True)) + epsilon)
    return (mixed * out_scale * post_gain[None, :]).astype(jnp.bfloat16)
```

```python
import jax
import jax.numpy as jnp
from jax import lax
from jax.experimental import pallas as pl
from jax.experimental.pallas import tpu as pltpu
from jax.sharding import Mesh
from jax.sharding import PartitionSpec as P

EP = ("ep_0", "ep_1", "ep_2")
CHIPS = ("ep_0", "ep_1")
epsilon = 1e-06
CAP = 3


def eye(n):
    return lax.broadcasted_iota(jnp.int32, (n, n), 0) == lax.broadcasted_iota(jnp.int32, (n, n), 1)


def to_col(row, diag):
    return jnp.sum(jnp.where(diag, row, 0.0), axis=1, keepdims=True)


def to_row(col, diag):
    return jnp.sum(jnp.where(diag, col, 0.0), axis=0, keepdims=True)


def pre_kernel(where_ref, tok_ref, gain_ref, ids_ref, out_ref, place_ref):
    rows, width = tok_ref.shape
    half = out_ref.shape[1]
    slots = out_ref.shape[0]
    parity = where_ref[0].astype(jnp.float32)
    start = pl.multiple_of(where_ref[1] * half, half)
    diag = eye(rows)
    lower = lax.broadcasted_iota(jnp.int32, (rows, rows), 0) < lax.broadcasted_iota(
        jnp.int32, (rows, rows), 1
    )
    ids = ids_ref[...].astype(jnp.float32)
    row0, row1 = ids[0:1, :], ids[1:2, :]
    col0, col1 = to_col(row0, diag), to_col(row1, diag)
    slot0 = jnp.sum(jnp.where((col0 == row0) & lower, 1.0, 0.0), axis=0, keepdims=True)
    slot1 = jnp.sum(jnp.where(col0 == row1, 1.0, 0.0), axis=0, keepdims=True) + jnp.sum(
        jnp.where((col1 == row1) & lower, 1.0, 0.0), axis=0, keepdims=True
    )
    chip0, chip1 = jnp.floor(row0 * 0.5), jnp.floor(row1 * 0.5)
    par0, par1 = row0 - 2.0 * chip0, row1 - 2.0 * chip1
    at0, at1 = CAP * chip0 + slot0, CAP * chip1 + slot1
    place_ref[0:1, :] = par0 * slots + at0
    place_ref[1:2, :] = par1 * slots + at1
    here0 = jnp.where(par0 == parity, at0, -1.0)
    here1 = jnp.where(par1 == parity, at1, -1.0)
    slot = lax.broadcasted_iota(jnp.int32, (slots, rows), 0).astype(jnp.float32)
    pick = jnp.where((slot == here0) | (slot == here1), 1.0, 0.0).astype(jnp.bfloat16)
    values = tok_ref[...].astype(jnp.float32)
    scale = lax.rsqrt(jnp.mean(values * values, axis=1, keepdims=True) + epsilon)
    part = tok_ref[:, pl.ds(start, half)].astype(jnp.float32)
    normed = (part * scale * gain_ref[:, pl.ds(start, half)]).astype(jnp.bfloat16)
    out_ref[...] = jnp.dot(pick, normed, preferred_element_type=jnp.float32).astype(jnp.bfloat16)


def hidden_kernel(where_ref, mine_ref, other_ref, g0, u0, g1, u1, g2, u2, out_ref):
    half = mine_ref.shape[1]
    ours = pl.multiple_of(where_ref[1] * half, half)
    theirs = pl.multiple_of((1 - where_ref[1]) * half, half)

    def work(ga, ua, gb, ub):
        def weights(at):
            rows = pl.ds(at, half)
            return jnp.concatenate(
                [ga[rows, :], gb[rows, :], ua[rows, :], ub[rows, :]], axis=1
            )

        sums = jnp.dot(mine_ref[...], weights(ours), preferred_element_type=jnp.float32)
        sums += jnp.dot(other_ref[...], weights(theirs), preferred_element_type=jnp.float32)
        cols = out_ref.shape[2]
        gate, up = sums[:, :cols], sums[:, cols:]
        hidden = (gate / (1.0 + jnp.exp(-gate)) * up).astype(jnp.bfloat16)
        for i in range(out_ref.shape[0]):
            out_ref[i] = hidden

    @pl.when(where_ref[2] == 1)
    def _():
        work(g0, u0, g1, u1)

    @pl.when(where_ref[2] == 0)
    def _():
        work(g1, u1, g2, u2)


def down_kernel(where_ref, hid_ref, mine_ref, other_ref, out_ref):
    slices = hid_ref.shape[0]
    wide = hid_ref.shape[2] // 2
    cols = mine_ref.shape[1]

    def work(first, second):
        for b, w in enumerate((first, second)):
            total = None
            for h in range(2):
                y = 2 * b + h
                for s, part in ((y, hid_ref[y, :, :wide]), (slices - 1 - y, hid_ref[y, :, wide:])):
                    add = jnp.dot(
                        part, w[s * wide : (s + 1) * wide, :], preferred_element_type=jnp.float32
                    )
                    total = add if total is None else total + add
            out_ref[:, b * cols : (b + 1) * cols] = total.astype(jnp.bfloat16)

    @pl.when(where_ref[3] == 0)
    def _():
        work(mine_ref, other_ref)

    @pl.when(where_ref[3] == 1)
    def _():
        work(other_ref, mine_ref)


def mix_kernel(back_ref, place_ref, weight_ref, mixed_ref, squares_ref):
    slots = back_ref.shape[0]
    rows, cols = mixed_ref.shape
    diag = eye(rows)
    lane = lax.broadcasted_iota(jnp.int32, (rows, slots), 1).astype(jnp.float32)
    mixed = None
    for k in range(2):
        place = to_col(place_ref[k : k + 1, :], diag)
        weight = to_col(weight_ref[k : k + 1, :], diag)
        picked = None
        for b in range(2):
            pick = jnp.where(lane + float(b * slots) == place, 1.0, 0.0).astype(jnp.bfloat16)
            add = jnp.dot(
                pick, back_ref[:, b * cols : (b + 1) * cols], preferred_element_type=jnp.float32
            )
            picked = add if picked is None else picked + add
        mixed = picked * weight if mixed is None else mixed + picked * weight
    mixed_ref[...] = mixed
    squares = to_row(jnp.sum(mixed * mixed, axis=1, keepdims=True), diag)
    squares_ref[...] = jnp.broadcast_to(squares[None], squares_ref.shape)


def norm_kernel(width, mixed_ref, squares_ref, gain_ref, out_ref):
    squares = jnp.sum(squares_ref[...], axis=0)[0:1, :]
    total = to_col(squares, eye(squares.shape[1]))
    scale = lax.rsqrt(total / width + epsilon)
    out_ref[...] = (mixed_ref[...] * scale * gain_ref[...]).astype(jnp.bfloat16)


SMEM = pl.BlockSpec(memory_space=pltpu.SMEM)
VMEM = pl.BlockSpec(memory_space=pltpu.VMEM)


def call(kernel, name, outs, *args, scalars=True):
    specs = [SMEM if scalars and i == 0 else VMEM for i in range(len(args))]
    return pl.pallas_call(
        kernel,
        name=name,
        out_shape=outs,
        in_specs=specs,
        out_specs=jax.tree.map(lambda _: VMEM, outs),
    )(*args)


def shape(dims, dtype):
    return jax.ShapeDtypeStruct(dims, dtype)


def per_device(tokens, pre_gain, post_gain, expert_ids, route_weights, w_gate, w_up, w_down):
    tok_rows, width = tokens.shape
    chips = lax.axis_size(CHIPS)
    tp = lax.axis_size("tp")
    slots = chips * CAP
    half = width // 2
    y, core = lax.axis_index("tp"), lax.axis_index("ep_2")
    parity = y // 2
    where = jnp.stack([parity, y % 2, (core == parity).astype(jnp.int32), core]).astype(jnp.int32)
    gate, up, down = w_gate[0], w_up[0], w_down[0]
    ff = gate.shape[1]
    cols = down.shape[1]

    buffer, place = call(
        pre_kernel,
        "pre",
        (shape((slots, half), jnp.bfloat16), shape((2, tok_rows), jnp.float32)),
        where,
        tokens,
        pre_gain[None, :],
        expert_ids.T,
    )

    def exchange(rows):
        pieces = rows.reshape(chips, slots * half // (chips * 128), 128)
        return lax.all_to_all(pieces, CHIPS, 0, 0, tiled=True)

    with jax.named_scope("dispatch"):
        arrived = exchange(buffer)

    first, second = [], []
    for c in range(2):
        for t in range(tp):
            b = t // 2
            source = c * tp + t
            if c == b:
                first.append((source, (1 - c) * tp + t))
            else:
                first.append((source, c * tp + tp - 1 - t))
                second.append((source, (1 - c) * tp + tp - 1 - t))
    with jax.named_scope("weights"):
        g1 = lax.ppermute(gate, ("ep_2", "tp"), first)
        u1 = lax.ppermute(up, ("ep_2", "tp"), first)
        g2 = lax.ppermute(gate, ("ep_2", "tp"), second)
        u2 = lax.ppermute(up, ("ep_2", "tp"), second)
        down_other = lax.ppermute(down, "ep_2", [(0, 1), (1, 0)])

    with jax.named_scope("pair"):
        theirs = lax.ppermute(arrived, "tp", [(t, t ^ 1) for t in range(tp)])

    hidden = call(
        hidden_kernel,
        "hidden",
        shape((tp, slots, 2 * ff), jnp.bfloat16),
        where,
        arrived.reshape(slots, half),
        theirs.reshape(slots, half),
        gate,
        up,
        g1,
        u1,
        g2,
        u2,
    )
    with jax.named_scope("gather"):
        hidden = lax.all_to_all(hidden, "tp", 0, 0, tiled=True)
    results = call(
        down_kernel, "down", shape((slots, 2 * cols), jnp.bfloat16), where, hidden, down, down_other
    )
    with jax.named_scope("back"):
        returned = exchange(results).reshape(slots, 2 * cols)
    mixed, squares = call(
        mix_kernel,
        "mix",
        (shape((tok_rows, cols), jnp.float32), shape((tp, 8, tok_rows), jnp.float32)),
        returned,
        place,
        route_weights.T,
        scalars=False,
    )
    with jax.named_scope("squares"):
        squares = lax.all_to_all(squares, "tp", 0, 0, tiled=True)
    return call(
        lambda *refs: norm_kernel(width, *refs),
        "norm",
        shape((tok_rows, cols), jnp.bfloat16),
        mixed,
        squares,
        post_gain[None, :],
        scalars=False,
    )


def solution(mesh):
    torus = Mesh(mesh.devices.reshape(16, 4, 2, mesh.shape["tp"]), ("ep_0", "ep_1", "ep_2", "tp"))
    in_specs = (
        P(EP, None),
        P(),
        P("tp"),
        P(EP, None),
        P(EP, None),
        P(EP, None, "tp"),
        P(EP, None, "tp"),
        P(EP, None, "tp"),
    )
    return jax.shard_map(
        per_device, mesh=torus, in_specs=in_specs, out_specs=P(EP, "tp"), check_vma=False
    )
```

```python
import jax
import jax.numpy as jnp
from jax import lax
from jax.experimental import pallas as pl
from jax.experimental.pallas import tpu as pltpu
from jax.sharding import Mesh
from jax.sharding import PartitionSpec as P

EP = ("ep_0", "ep_1", "ep_2")
CHIPS = ("ep_0", "ep_1")
epsilon = 1e-06
CAP = 3


def eye(n):
    return lax.broadcasted_iota(jnp.int32, (n, n), 0) == lax.broadcasted_iota(jnp.int32, (n, n), 1)


def to_col(row, diag):
    return jnp.sum(jnp.where(diag, row, 0.0), axis=1, keepdims=True)


def to_row(col, diag):
    return jnp.sum(jnp.where(diag, col, 0.0), axis=0, keepdims=True)


def spread(pieces_ref, scratch_ref):
    scratch_ref[...] = pieces_ref[...].astype(jnp.float32)
    return [chunk(scratch_ref, k)[...].astype(jnp.bfloat16) for k in range(CHUNKS)]


def chunk(scratch_ref, k):
    return scratch_ref.at[pl.ds(k, scratch_ref.shape[0] // CHUNKS, stride=CHUNKS), :]


def gathered(scratch_ref, out_ref):
    out_ref[...] = scratch_ref[...].astype(jnp.bfloat16)


def pre_kernel(tok_ref, gain_ref, ids_ref, out_ref, place_ref, scratch_ref):
    rows, width = tok_ref.shape
    half = CHUNKS * 128
    slots = out_ref.shape[0] // CHUNKS
    y = lax.axis_index("tp")
    parity = (y // 2).astype(jnp.float32)
    start = pl.multiple_of((y % 2) * half, half)
    diag = eye(rows)
    lower = lax.broadcasted_iota(jnp.int32, (rows, rows), 0) < lax.broadcasted_iota(
        jnp.int32, (rows, rows), 1
    )
    ids = ids_ref[...].astype(jnp.float32)
    row0, row1 = ids[0:1, :], ids[1:2, :]
    col0, col1 = to_col(row0, diag), to_col(row1, diag)
    slot0 = jnp.sum(jnp.where((col0 == row0) & lower, 1.0, 0.0), axis=0, keepdims=True)
    slot1 = jnp.sum(jnp.where(col0 == row1, 1.0, 0.0), axis=0, keepdims=True) + jnp.sum(
        jnp.where((col1 == row1) & lower, 1.0, 0.0), axis=0, keepdims=True
    )
    chip0, chip1 = jnp.floor(row0 * 0.5), jnp.floor(row1 * 0.5)
    par0, par1 = row0 - 2.0 * chip0, row1 - 2.0 * chip1
    at0, at1 = CAP * chip0 + slot0, CAP * chip1 + slot1
    place_ref[0:1, :] = par0 * slots + at0
    place_ref[1:2, :] = par1 * slots + at1
    here0 = jnp.where(par0 == parity, at0, -1.0)
    here1 = jnp.where(par1 == parity, at1, -1.0)
    slot = lax.broadcasted_iota(jnp.int32, (slots, rows), 0).astype(jnp.float32)
    pick = jnp.where((slot == here0) | (slot == here1), 1.0, 0.0).astype(jnp.bfloat16)
    values = tok_ref[...].astype(jnp.float32)
    scale = lax.rsqrt(jnp.mean(values * values, axis=1, keepdims=True) + epsilon)
    part = tok_ref[:, pl.ds(start, half)].astype(jnp.float32)
    normed = (part * scale * gain_ref[:, pl.ds(start, half)]).astype(jnp.bfloat16)
    sent = jnp.dot(pick, normed, preferred_element_type=jnp.float32)
    for k in range(CHUNKS):
        chunk(scratch_ref, k)[...] = sent[:, k * 128 : (k + 1) * 128]
    gathered(scratch_ref, out_ref)


def up_sums(pieces_ref, part, scratch_ref, g0, u0, g1, u1, g2, u2, finish):
    half = CHUNKS * 128
    start = pl.multiple_of(part * half, half)
    mine = lax.axis_index("ep_2") == lax.axis_index("tp") // 2
    rows = jnp.concatenate(spread(pieces_ref, scratch_ref), axis=1)

    def work(*weights):
        columns = jnp.concatenate([w[pl.ds(start, half), :] for w in weights], axis=1)
        finish(jnp.dot(rows, columns, preferred_element_type=jnp.float32))

    @pl.when(mine)
    def _():
        work(g0, g1, u0, u1)

    @pl.when(jnp.logical_not(mine))
    def _():
        work(g1, g2, u1, u2)


def first_kernel(pieces_ref, g0, u0, g1, u1, g2, u2, sums_ref, scratch_ref):
    def finish(sums):
        sums_ref[...] = sums

    part = lax.axis_index("tp") % 2
    up_sums(pieces_ref, part, scratch_ref, g0, u0, g1, u1, g2, u2, finish)


def hidden_kernel(pieces_ref, sums_ref, g0, u0, g1, u1, g2, u2, out_ref, scratch_ref):
    def finish(sums):
        sums = sums_ref[...] + sums
        cols = out_ref.shape[2]
        gate, up = sums[:, :cols], sums[:, cols:]
        hidden = (gate / (1.0 + jnp.exp(-gate)) * up).astype(jnp.bfloat16)
        for i in range(out_ref.shape[0]):
            out_ref[i] = hidden

    part = 1 - lax.axis_index("tp") % 2
    up_sums(pieces_ref, part, scratch_ref, g0, u0, g1, u1, g2, u2, finish)


def down_kernel(hid_ref, mine_ref, other_ref, out_ref, scratch_ref):
    core = lax.axis_index("ep_2")
    slices = hid_ref.shape[0]
    wide = hid_ref.shape[2] // 2
    cols = mine_ref.shape[1]

    def work(first, second):
        for b, w in enumerate((first, second)):
            total = None
            for h in range(2):
                y = 2 * b + h
                for s, part in ((y, hid_ref[y, :, :wide]), (slices - 1 - y, hid_ref[y, :, wide:])):
                    add = jnp.dot(
                        part, w[s * wide : (s + 1) * wide, :], preferred_element_type=jnp.float32
                    )
                    total = add if total is None else total + add
            per = CHUNKS // 2
            for k in range(per):
                chunk(scratch_ref, b * per + k)[...] = total[:, k * 128 : (k + 1) * 128]

    @pl.when(core == 0)
    def _():
        work(mine_ref, other_ref)

    @pl.when(core == 1)
    def _():
        work(other_ref, mine_ref)

    gathered(scratch_ref, out_ref)


def mix_kernel(back_ref, place_ref, weight_ref, mixed_ref, squares_ref, scratch_ref):
    slots = back_ref.shape[0] // CHUNKS
    rows, cols = mixed_ref.shape
    diag = eye(rows)
    lane = lax.broadcasted_iota(jnp.int32, (rows, slots), 1).astype(jnp.float32)
    pieces = spread(back_ref, scratch_ref)
    per = CHUNKS // 2
    back = [jnp.concatenate(pieces[b * per : (b + 1) * per], axis=1) for b in range(2)]
    mixed = None
    for k in range(2):
        place = to_col(place_ref[k : k + 1, :], diag)
        weight = to_col(weight_ref[k : k + 1, :], diag)
        picked = None
        for b in range(2):
            pick = jnp.where(lane + float(b * slots) == place, 1.0, 0.0).astype(jnp.bfloat16)
            add = jnp.dot(pick, back[b], preferred_element_type=jnp.float32)
            picked = add if picked is None else picked + add
        mixed = picked * weight if mixed is None else mixed + picked * weight
    mixed_ref[...] = mixed
    squares = to_row(jnp.sum(mixed * mixed, axis=1, keepdims=True), diag)
    squares_ref[...] = jnp.broadcast_to(squares[None], squares_ref.shape)


def norm_kernel(width, mixed_ref, squares_ref, gain_ref, out_ref):
    squares = jnp.sum(squares_ref[...], axis=0)[0:1, :]
    total = to_col(squares, eye(squares.shape[1]))
    scale = lax.rsqrt(total / width + epsilon)
    out_ref[...] = (mixed_ref[...] * scale * gain_ref[...]).astype(jnp.bfloat16)


CHUNKS = 8
WHOLE = pl.BlockSpec(memory_space=pltpu.VMEM)


def call(kernel, name, outs, *args, scratch=None, outside=()):
    args = [
        a if i in outside else pltpu.with_memory_space_constraint(a, pltpu.VMEM)
        for i, a in enumerate(args)
    ]
    return pl.pallas_call(
        kernel,
        name=name,
        out_shape=outs,
        in_specs=[WHOLE] * len(args),
        out_specs=jax.tree.map(lambda _: WHOLE, outs, is_leaf=lambda o: hasattr(o, "dtype")),
        compiler_params=pltpu.CompilerParams(vmem_limit_bytes=16 << 20),
        scratch_shapes=[] if scratch is None else [pltpu.VMEM(scratch, jnp.float32)],
    )(*args)


def near(dims, dtype):
    return pltpu.VMEM(dims, dtype)


def per_device(tokens, pre_gain, post_gain, expert_ids, route_weights, w_gate, w_up, w_down):
    tok_rows, width = tokens.shape
    chips = lax.axis_size(CHIPS)
    tp = lax.axis_size("tp")
    slots = chips * CAP
    gate, up, down = w_gate[0], w_up[0], w_down[0]
    ff = gate.shape[1]
    cols = down.shape[1]
    flat = (slots * CHUNKS, 128)

    buffer, place = call(
        pre_kernel,
        "pre",
        (near(flat, jnp.bfloat16), near((2, tok_rows), jnp.float32)),
        tokens,
        pre_gain[None, :],
        expert_ids.T,
        scratch=flat,
        outside=(0, 1, 2),
    )

    def exchange(rows):
        pieces = rows.reshape(chips, CAP * CHUNKS, 128)
        return lax.all_to_all(pieces, CHIPS, 0, 0, tiled=True).reshape(flat)

    with jax.named_scope("dispatch"):
        arrived = exchange(buffer)

    first, second = [], []
    for c in range(2):
        for t in range(tp):
            b = t // 2
            source = c * tp + t
            if c == b:
                first.append((source, (1 - c) * tp + t))
            else:
                first.append((source, c * tp + tp - 1 - t))
                second.append((source, (1 - c) * tp + tp - 1 - t))
    with jax.named_scope("weights"):
        g1 = lax.ppermute(gate, ("ep_2", "tp"), first)
        u1 = lax.ppermute(up, ("ep_2", "tp"), first)
        g2 = lax.ppermute(gate, ("ep_2", "tp"), second)
        u2 = lax.ppermute(up, ("ep_2", "tp"), second)
        down_other = lax.ppermute(down, "ep_2", [(0, 1), (1, 0)])

    arrived, down_other = lax.optimization_barrier((arrived, down_other))
    with jax.named_scope("pair"):
        theirs = lax.ppermute(arrived, "tp", [(t, t ^ 1) for t in range(tp)])
    weights = (gate, up, g1, u1, g2, u2)
    sums = call(
        first_kernel, "first", near((slots, 4 * ff), jnp.float32), arrived, *weights, scratch=flat
    )
    hidden = call(
        hidden_kernel,
        "hidden",
        near((tp, slots, 2 * ff), jnp.bfloat16),
        theirs,
        sums,
        *weights,
        scratch=flat,
    )
    with jax.named_scope("gather"):
        hidden = lax.all_to_all(hidden, "tp", 0, 0, tiled=True)
    results = call(
        down_kernel, "down", near(flat, jnp.bfloat16), hidden, down, down_other, scratch=flat
    )
    with jax.named_scope("back"):
        returned = exchange(results)
    mixed, squares = call(
        mix_kernel,
        "mix",
        (near((tok_rows, cols), jnp.float32), near((tp, 8, tok_rows), jnp.float32)),
        returned,
        place,
        route_weights.T,
        scratch=flat,
        outside=(2,),
    )
    with jax.named_scope("squares"):
        squares = lax.all_to_all(squares, "tp", 0, 0, tiled=True)
    return call(
        lambda *refs: norm_kernel(width, *refs),
        "norm",
        jax.ShapeDtypeStruct((tok_rows, cols), jnp.bfloat16),
        mixed,
        squares,
        post_gain[None, :],
        outside=(2,),
    )


def solution(mesh):
    torus = Mesh(mesh.devices.reshape(16, 4, 2, mesh.shape["tp"]), ("ep_0", "ep_1", "ep_2", "tp"))
    in_specs = (
        P(EP, None),
        P(),
        P("tp"),
        P(EP, None),
        P(EP, None),
        P(EP, None, "tp"),
        P(EP, None, "tp"),
        P(EP, None, "tp"),
    )
    return jax.shard_map(
        per_device, mesh=torus, in_specs=in_specs, out_specs=P(EP, "tp"), check_vma=False
    )
```

```python
import jax
import jax.numpy as jnp
from jax import lax
from jax.experimental import pallas as pl
from jax.experimental.pallas import tpu as pltpu
from jax.sharding import Mesh
from jax.sharding import PartitionSpec as P

EP = ("ep_0", "ep_1", "ep_2")
CHIPS = ("ep_0", "ep_1")
epsilon = 1e-06
CAP = 3


def eye(n):
    return lax.broadcasted_iota(jnp.int32, (n, n), 0) == lax.broadcasted_iota(jnp.int32, (n, n), 1)


def to_col(row, diag):
    return jnp.sum(jnp.where(diag, row, 0.0), axis=1, keepdims=True)


def to_row(col, diag):
    return jnp.sum(jnp.where(diag, col, 0.0), axis=0, keepdims=True)


def spread(pieces_ref, scratch_ref):
    scratch_ref[...] = pieces_ref[...].astype(jnp.float32)
    return [chunk(scratch_ref, k)[...].astype(jnp.bfloat16) for k in range(CHUNKS)]


def chunk(scratch_ref, k):
    return scratch_ref.at[pl.ds(k, scratch_ref.shape[0] // CHUNKS, stride=CHUNKS), :]


def gathered(scratch_ref, out_ref):
    out_ref[...] = scratch_ref[...].astype(jnp.bfloat16)


def pre_kernel(
    tok_hbm,
    gain_hbm,
    ids_hbm,
    weight_hbm,
    post_hbm,
    out_ref,
    place_ref,
    weight_ref,
    post_ref,
    scratch_ref,
    tok_ref,
    gain_ref,
    ids_ref,
    sems,
):
    rows, width = tok_ref.shape
    half = CHUNKS * 128
    slots = out_ref.shape[0] // CHUNKS
    block = rows // PARTS
    pieces = [(ids_hbm, ids_ref)]
    for i in range(PARTS):
        span = pl.ds(i * block, block)
        pieces.append((tok_hbm.at[span, :], tok_ref.at[span, :]))
    pieces += [(gain_hbm, gain_ref), (weight_hbm, weight_ref), (post_hbm, post_ref)]
    copies = [pltpu.make_async_copy(a, b, sems.at[i]) for i, (a, b) in enumerate(pieces)]
    for copy in copies:
        copy.start()
    y = lax.axis_index("tp")
    parity = (y // 2).astype(jnp.float32)
    start = pl.multiple_of((y % 2) * half, half)
    diag = eye(rows)
    lower = lax.broadcasted_iota(jnp.int32, (rows, rows), 0) < lax.broadcasted_iota(
        jnp.int32, (rows, rows), 1
    )
    copies[0].wait()
    ids = ids_ref[...].astype(jnp.float32)
    row0, row1 = ids[0:1, :], ids[1:2, :]
    col0, col1 = to_col(row0, diag), to_col(row1, diag)
    slot0 = jnp.sum(jnp.where((col0 == row0) & lower, 1.0, 0.0), axis=0, keepdims=True)
    slot1 = jnp.sum(jnp.where(col0 == row1, 1.0, 0.0), axis=0, keepdims=True) + jnp.sum(
        jnp.where((col1 == row1) & lower, 1.0, 0.0), axis=0, keepdims=True
    )
    chip0, chip1 = jnp.floor(row0 * 0.5), jnp.floor(row1 * 0.5)
    par0, par1 = row0 - 2.0 * chip0, row1 - 2.0 * chip1
    at0, at1 = CAP * chip0 + slot0, CAP * chip1 + slot1
    place_ref[0:1, :] = par0 * slots + at0
    place_ref[1:2, :] = par1 * slots + at1
    here0 = jnp.where(par0 == parity, at0, -1.0)
    here1 = jnp.where(par1 == parity, at1, -1.0)
    slot = lax.broadcasted_iota(jnp.int32, (slots, rows), 0).astype(jnp.float32)
    pick = jnp.where((slot == here0) | (slot == here1), 1.0, 0.0).astype(jnp.bfloat16)
    copies[PARTS + 1].wait()
    gain = gain_ref[:, pl.ds(start, half)]
    normed = []
    for i in range(PARTS):
        span = pl.ds(i * block, block)
        copies[1 + i].wait()
        values = tok_ref[span, :].astype(jnp.float32)
        scale = lax.rsqrt(jnp.mean(values * values, axis=1, keepdims=True) + epsilon)
        part = tok_ref[span, pl.ds(start, half)].astype(jnp.float32)
        normed.append((part * scale * gain).astype(jnp.bfloat16))
    normed = jnp.concatenate(normed, axis=0)
    sent = jnp.dot(pick, normed, preferred_element_type=jnp.float32)
    for k in range(CHUNKS):
        chunk(scratch_ref, k)[...] = sent[:, k * 128 : (k + 1) * 128]
    gathered(scratch_ref, out_ref)
    copies[PARTS + 2].wait()
    copies[PARTS + 3].wait()


def up_sums(pieces_ref, part, scratch_ref, g0, u0, g1, u1, g2, u2, finish):
    half = CHUNKS * 128
    start = pl.multiple_of(part * half, half)
    mine = lax.axis_index("ep_2") == lax.axis_index("tp") // 2
    rows = jnp.concatenate(spread(pieces_ref, scratch_ref), axis=1)

    def work(*weights):
        columns = jnp.concatenate([w[pl.ds(start, half), :] for w in weights], axis=1)
        finish(jnp.dot(rows, columns, preferred_element_type=jnp.float32))

    @pl.when(mine)
    def _():
        work(g0, g1, u0, u1)

    @pl.when(jnp.logical_not(mine))
    def _():
        work(g1, g2, u1, u2)


def first_kernel(pieces_ref, g0, u0, g1, u1, g2, u2, sums_ref, scratch_ref):
    def finish(sums):
        sums_ref[...] = sums

    part = lax.axis_index("tp") % 2
    up_sums(pieces_ref, part, scratch_ref, g0, u0, g1, u1, g2, u2, finish)


def hidden_kernel(pieces_ref, sums_ref, g0, u0, g1, u1, g2, u2, out_ref, scratch_ref):
    def finish(sums):
        sums = sums_ref[...] + sums
        cols = out_ref.shape[2]
        gate, up = sums[:, :cols], sums[:, cols:]
        hidden = (gate / (1.0 + jnp.exp(-gate)) * up).astype(jnp.bfloat16)
        for i in range(out_ref.shape[0]):
            out_ref[i] = hidden

    part = 1 - lax.axis_index("tp") % 2
    up_sums(pieces_ref, part, scratch_ref, g0, u0, g1, u1, g2, u2, finish)


def down_kernel(hid_ref, mine_ref, other_ref, out_ref, scratch_ref):
    core = lax.axis_index("ep_2")
    slices = hid_ref.shape[0]
    wide = hid_ref.shape[2] // 2
    cols = mine_ref.shape[1]

    def work(first, second):
        for b, w in enumerate((first, second)):
            total = None
            for h in range(2):
                y = 2 * b + h
                for s, part in ((y, hid_ref[y, :, :wide]), (slices - 1 - y, hid_ref[y, :, wide:])):
                    add = jnp.dot(
                        part, w[s * wide : (s + 1) * wide, :], preferred_element_type=jnp.float32
                    )
                    total = add if total is None else total + add
            per = CHUNKS // 2
            for k in range(per):
                chunk(scratch_ref, b * per + k)[...] = total[:, k * 128 : (k + 1) * 128]

    @pl.when(core == 0)
    def _():
        work(mine_ref, other_ref)

    @pl.when(core == 1)
    def _():
        work(other_ref, mine_ref)

    gathered(scratch_ref, out_ref)


def mix_kernel(back_ref, place_ref, weight_ref, mixed_ref, squares_ref, scratch_ref):
    slots = back_ref.shape[0] // CHUNKS
    rows, cols = mixed_ref.shape
    diag = eye(rows)
    lane = lax.broadcasted_iota(jnp.int32, (rows, slots), 1).astype(jnp.float32)
    pieces = spread(back_ref, scratch_ref)
    per = CHUNKS // 2
    back = [jnp.concatenate(pieces[b * per : (b + 1) * per], axis=1) for b in range(2)]
    mixed = None
    for k in range(2):
        place = to_col(place_ref[k : k + 1, :], diag)
        weight = to_col(weight_ref[k : k + 1, :], diag)
        picked = None
        for b in range(2):
            pick = jnp.where(lane + float(b * slots) == place, 1.0, 0.0).astype(jnp.bfloat16)
            add = jnp.dot(pick, back[b], preferred_element_type=jnp.float32)
            picked = add if picked is None else picked + add
        mixed = picked * weight if mixed is None else mixed + picked * weight
    mixed_ref[...] = mixed
    squares = to_row(jnp.sum(mixed * mixed, axis=1, keepdims=True), diag)
    squares_ref[...] = jnp.broadcast_to(squares[None], squares_ref.shape)


def norm_kernel(width, mixed_ref, squares_ref, gain_ref, out_ref):
    squares = jnp.sum(squares_ref[...], axis=0)[0:1, :]
    total = to_col(squares, eye(squares.shape[1]))
    scale = lax.rsqrt(total / width + epsilon)
    out_ref[...] = (mixed_ref[...] * scale * gain_ref[...]).astype(jnp.bfloat16)


CHUNKS = 8
PARTS = 4
WHOLE = pl.BlockSpec(memory_space=pltpu.VMEM)


def call(kernel, name, outs, *args, scratch=None):
    args = [pltpu.with_memory_space_constraint(a, pltpu.VMEM) for a in args]
    return pl.pallas_call(
        kernel,
        name=name,
        out_shape=outs,
        in_specs=[WHOLE] * len(args),
        out_specs=jax.tree.map(lambda _: WHOLE, outs, is_leaf=lambda o: hasattr(o, "dtype")),
        compiler_params=pltpu.CompilerParams(vmem_limit_bytes=16 << 20),
        scratch_shapes=[] if scratch is None else [pltpu.VMEM(scratch, jnp.float32)],
    )(*args)


def near(dims, dtype):
    return pltpu.VMEM(dims, dtype)


def per_device(tokens, pre_gain, post_gain, expert_ids, route_weights, w_gate, w_up, w_down):
    tok_rows, width = tokens.shape
    chips = lax.axis_size(CHIPS)
    tp = lax.axis_size("tp")
    slots = chips * CAP
    gate, up, down = w_gate[0], w_up[0], w_down[0]
    ff = gate.shape[1]
    cols = down.shape[1]
    flat = (slots * CHUNKS, 128)

    far = pl.BlockSpec(memory_space=pl.ANY)
    inputs = (tokens, pre_gain[None, :], expert_ids.T, route_weights.T, post_gain[None, :])
    buffer, place, mixing, post = pl.pallas_call(
        pre_kernel,
        name="pre",
        out_shape=(
            near(flat, jnp.bfloat16),
            near((2, tok_rows), jnp.float32),
            near((2, tok_rows), jnp.float32),
            near((1, cols), jnp.float32),
        ),
        in_specs=[far] * len(inputs),
        out_specs=(WHOLE,) * 4,
        compiler_params=pltpu.CompilerParams(vmem_limit_bytes=16 << 20),
        scratch_shapes=[
            pltpu.VMEM(flat, jnp.float32),
            pltpu.VMEM(tokens.shape, tokens.dtype),
            pltpu.VMEM(inputs[1].shape, jnp.float32),
            pltpu.VMEM(inputs[2].shape, jnp.int32),
            pltpu.SemaphoreType.DMA((PARTS + 4,)),
        ],
    )(*[pltpu.with_memory_space_constraint(a, pltpu.HBM) for a in inputs])

    def exchange(rows):
        pieces = rows.reshape(chips, CAP * CHUNKS, 128)
        return lax.all_to_all(pieces, CHIPS, 0, 0, tiled=True).reshape(flat)

    with jax.named_scope("dispatch"):
        arrived = exchange(buffer)

    first, second = [], []
    for c in range(2):
        for t in range(tp):
            b = t // 2
            source = c * tp + t
            if c == b:
                first.append((source, (1 - c) * tp + t))
            else:
                first.append((source, c * tp + tp - 1 - t))
                second.append((source, (1 - c) * tp + tp - 1 - t))
    with jax.named_scope("weights"):
        g1 = lax.ppermute(gate, ("ep_2", "tp"), first)
        u1 = lax.ppermute(up, ("ep_2", "tp"), first)
        g2 = lax.ppermute(gate, ("ep_2", "tp"), second)
        u2 = lax.ppermute(up, ("ep_2", "tp"), second)
        down_other = lax.ppermute(down, "ep_2", [(0, 1), (1, 0)])

    arrived, down_other = lax.optimization_barrier((arrived, down_other))
    with jax.named_scope("pair"):
        theirs = lax.ppermute(arrived, "tp", [(t, t ^ 1) for t in range(tp)])
    weights = (gate, up, g1, u1, g2, u2)
    sums = call(
        first_kernel, "first", near((slots, 4 * ff), jnp.float32), arrived, *weights, scratch=flat
    )
    hidden = call(
        hidden_kernel,
        "hidden",
        near((tp, slots, 2 * ff), jnp.bfloat16),
        theirs,
        sums,
        *weights,
        scratch=flat,
    )
    with jax.named_scope("gather"):
        hidden = lax.all_to_all(hidden, "tp", 0, 0, tiled=True)
    results = call(
        down_kernel, "down", near(flat, jnp.bfloat16), hidden, down, down_other, scratch=flat
    )
    with jax.named_scope("back"):
        returned = exchange(results)
    mixed, squares = call(
        mix_kernel,
        "mix",
        (near((tok_rows, cols), jnp.float32), near((tp, 8, tok_rows), jnp.float32)),
        returned,
        place,
        mixing,
        scratch=flat,
    )
    with jax.named_scope("squares"):
        squares = lax.all_to_all(squares, "tp", 0, 0, tiled=True)
    return call(
        lambda *refs: norm_kernel(width, *refs),
        "norm",
        jax.ShapeDtypeStruct((tok_rows, cols), jnp.bfloat16),
        mixed,
        squares,
        post,
    )


def solution(mesh):
    torus = Mesh(mesh.devices.reshape(16, 4, 2, mesh.shape["tp"]), ("ep_0", "ep_1", "ep_2", "tp"))
    in_specs = (
        P(EP, None),
        P(),
        P("tp"),
        P(EP, None),
        P(EP, None),
        P(EP, None, "tp"),
        P(EP, None, "tp"),
        P(EP, None, "tp"),
    )
    return jax.shard_map(
        per_device, mesh=torus, in_specs=in_specs, out_specs=P(EP, "tp"), check_vma=False
    )
```

```python
import jax
import jax.numpy as jnp
from jax import lax
from jax.experimental import pallas as pl
from jax.experimental.pallas import tpu as pltpu
from jax.sharding import Mesh
from jax.sharding import PartitionSpec as P

EP = ("ep_0", "ep_1", "ep_2")
CHIPS = ("ep_0", "ep_1")
epsilon = 1e-06
CAP = 3


def eye(n):
    return lax.broadcasted_iota(jnp.int32, (n, n), 0) == lax.broadcasted_iota(jnp.int32, (n, n), 1)


def to_col(row, diag):
    return jnp.sum(jnp.where(diag, row, 0.0), axis=1, keepdims=True)


def to_row(col, diag):
    return jnp.sum(jnp.where(diag, col, 0.0), axis=0, keepdims=True)


def role(core, y):
    parity = jnp.where(core == 0, y // 2, (y + y // 2) % 2)
    half = jnp.where(core == 0, y % 2, y // 2)
    return parity, half


def partner(core, y, tp):
    return y ^ 1 if core == 0 else tp - 1 - y


def neighbour(core, y, tp):
    return partner(1 - core, y, tp)


def weight_moves(tp):
    edges = []
    for c in range(2):
        for y in range(tp):
            parity = y // 2 if c == 0 else (y + y // 2) % 2
            for n, s in enumerate((y, neighbour(c, y, tp))):
                if (parity, s) != (c, y):
                    edges.append(((parity, s), (c, y), n))
    color = {}

    def fits(i, r):
        return all(
            color[j] != r or (edges[j][0] != edges[i][0] and edges[j][1] != edges[i][1])
            for j in color
            if j != i
        )

    def place(i):
        if i == len(edges):
            return True
        for r in (1, 2):
            if fits(i, r):
                color[i] = r
                if place(i + 1):
                    return True
                del color[i]
        return False

    assert place(0)
    rounds = [[], []]
    comes = {(c, y): [0, 0] for c in range(2) for y in range(tp)}
    for i, (source, target, n) in enumerate(edges):
        rounds[color[i] - 1].append((source[0] * tp + source[1], target[0] * tp + target[1]))
        comes[target][n] = color[i]
    return rounds, comes


def spread(pieces_ref, scratch_ref):
    scratch_ref[...] = pieces_ref[...].astype(jnp.float32)
    return [chunk(scratch_ref, k)[...].astype(jnp.bfloat16) for k in range(CHUNKS)]


def chunk(scratch_ref, k):
    return scratch_ref.at[pl.ds(k, scratch_ref.shape[0] // CHUNKS, stride=CHUNKS), :]


def gathered(scratch_ref, out_ref):
    out_ref[...] = scratch_ref[...].astype(jnp.bfloat16)


def pre_kernel(
    tok_hbm,
    gain_hbm,
    ids_hbm,
    weight_hbm,
    post_hbm,
    out_ref,
    place_ref,
    weight_ref,
    post_ref,
    scratch_ref,
    tok_ref,
    gain_ref,
    ids_ref,
    sems,
):
    rows, width = tok_ref.shape
    half = CHUNKS * 128
    slots = out_ref.shape[0] // CHUNKS
    block = rows // PARTS
    pieces = [(ids_hbm, ids_ref)]
    for i in range(PARTS):
        span = pl.ds(i * block, block)
        pieces.append((tok_hbm.at[span, :], tok_ref.at[span, :]))
    pieces += [(gain_hbm, gain_ref), (weight_hbm, weight_ref), (post_hbm, post_ref)]
    copies = [pltpu.make_async_copy(a, b, sems.at[i]) for i, (a, b) in enumerate(pieces)]
    for copy in copies:
        copy.start()
    parity, side = role(lax.axis_index("ep_2"), lax.axis_index("tp"))
    parity = parity.astype(jnp.float32)
    start = pl.multiple_of(side * half, half)
    diag = eye(rows)
    lower = lax.broadcasted_iota(jnp.int32, (rows, rows), 0) < lax.broadcasted_iota(
        jnp.int32, (rows, rows), 1
    )
    copies[0].wait()
    ids = ids_ref[...].astype(jnp.float32)
    row0, row1 = ids[0:1, :], ids[1:2, :]
    col0, col1 = to_col(row0, diag), to_col(row1, diag)
    slot0 = jnp.sum(jnp.where((col0 == row0) & lower, 1.0, 0.0), axis=0, keepdims=True)
    slot1 = jnp.sum(jnp.where(col0 == row1, 1.0, 0.0), axis=0, keepdims=True) + jnp.sum(
        jnp.where((col1 == row1) & lower, 1.0, 0.0), axis=0, keepdims=True
    )
    chip0, chip1 = jnp.floor(row0 * 0.5), jnp.floor(row1 * 0.5)
    par0, par1 = row0 - 2.0 * chip0, row1 - 2.0 * chip1
    at0, at1 = CAP * chip0 + slot0, CAP * chip1 + slot1
    place_ref[0:1, :] = par0 * slots + at0
    place_ref[1:2, :] = par1 * slots + at1
    here0 = jnp.where(par0 == parity, at0, -1.0)
    here1 = jnp.where(par1 == parity, at1, -1.0)
    slot = lax.broadcasted_iota(jnp.int32, (slots, rows), 0).astype(jnp.float32)
    pick = jnp.where((slot == here0) | (slot == here1), 1.0, 0.0).astype(jnp.bfloat16)
    copies[PARTS + 1].wait()
    gain = gain_ref[:, pl.ds(start, half)]
    normed = []
    for i in range(PARTS):
        span = pl.ds(i * block, block)
        copies[1 + i].wait()
        values = tok_ref[span, :].astype(jnp.float32)
        scale = lax.rsqrt(jnp.mean(values * values, axis=1, keepdims=True) + epsilon)
        part = tok_ref[span, pl.ds(start, half)].astype(jnp.float32)
        normed.append((part * scale * gain).astype(jnp.bfloat16))
    normed = jnp.concatenate(normed, axis=0)
    sent = jnp.dot(pick, normed, preferred_element_type=jnp.float32)
    for k in range(CHUNKS):
        chunk(scratch_ref, k)[...] = sent[:, k * 128 : (k + 1) * 128]
    gathered(scratch_ref, out_ref)
    copies[PARTS + 2].wait()
    copies[PARTS + 3].wait()


def up_sums(pieces_ref, other, scratch_ref, weights, finish):
    half = CHUNKS * 128
    core, y = lax.axis_index("ep_2"), lax.axis_index("tp")
    side = role(core, y)[1]
    start = pl.multiple_of((1 - side if other else side) * half, half)
    rows = jnp.concatenate(spread(pieces_ref, scratch_ref), axis=1)

    def work(first, second):
        chosen = (*(weights[2 * r] for r in (first, second)), *(weights[2 * r + 1] for r in (first, second)))
        columns = jnp.concatenate([w[pl.ds(start, half), :] for w in chosen], axis=1)
        finish(jnp.dot(rows, columns, preferred_element_type=jnp.float32))

    cases = {}
    for (c, t), comes in weight_moves(lax.axis_size("tp"))[1].items():
        cases.setdefault(tuple(comes), []).append((core == c) & (y == t))
    for comes, devices in sorted(cases.items()):
        here = devices[0]
        for device in devices[1:]:
            here = here | device
        pl.when(here)(lambda comes=comes: work(*comes))


def first_kernel(pieces_ref, g0, u0, g1, u1, g2, u2, sums_ref, scratch_ref):
    def finish(sums):
        sums_ref[...] = sums

    up_sums(pieces_ref, False, scratch_ref, (g0, u0, g1, u1, g2, u2), finish)


def hidden_kernel(pieces_ref, sums_ref, g0, u0, g1, u1, g2, u2, out_ref, scratch_ref):
    def finish(sums):
        sums = sums_ref[...] + sums
        cols = out_ref.shape[2]
        gate, up = sums[:, :cols], sums[:, cols:]
        hidden = (gate / (1.0 + jnp.exp(-gate)) * up).astype(jnp.bfloat16)
        for i in range(out_ref.shape[0]):
            out_ref[i] = hidden

    up_sums(pieces_ref, True, scratch_ref, (g0, u0, g1, u1, g2, u2), finish)


def down_kernel(hid_ref, mine_ref, other_ref, out_ref, scratch_ref):
    core = lax.axis_index("ep_2")
    slices = hid_ref.shape[0]
    wide = hid_ref.shape[2] // 2
    cols = mine_ref.shape[1]
    per = CHUNKS // 2

    def work(c, weights):
        for b, w in enumerate(weights):
            total = None
            for y in range(slices):
                if (y // 2 if c == 0 else (y + y // 2) % 2) != b:
                    continue
                for n, s in enumerate((y, neighbour(c, y, slices))):
                    add = jnp.dot(
                        hid_ref[y, :, n * wide : (n + 1) * wide],
                        w[s * wide : (s + 1) * wide, :],
                        preferred_element_type=jnp.float32,
                    )
                    total = add if total is None else total + add
            for k in range(per):
                chunk(scratch_ref, b * per + k)[...] = total[:, k * 128 : (k + 1) * 128]

    @pl.when(core == 0)
    def _():
        work(0, (mine_ref, other_ref))

    @pl.when(core == 1)
    def _():
        work(1, (other_ref, mine_ref))

    gathered(scratch_ref, out_ref)


def mix_kernel(back_ref, place_ref, weight_ref, mixed_ref, squares_ref, scratch_ref):
    slots = back_ref.shape[0] // CHUNKS
    rows, cols = mixed_ref.shape
    diag = eye(rows)
    lane = lax.broadcasted_iota(jnp.int32, (rows, slots), 1).astype(jnp.float32)
    pieces = spread(back_ref, scratch_ref)
    per = CHUNKS // 2
    back = [jnp.concatenate(pieces[b * per : (b + 1) * per], axis=1) for b in range(2)]
    mixed = None
    for k in range(2):
        place = to_col(place_ref[k : k + 1, :], diag)
        weight = to_col(weight_ref[k : k + 1, :], diag)
        picked = None
        for b in range(2):
            pick = jnp.where(lane + float(b * slots) == place, 1.0, 0.0).astype(jnp.bfloat16)
            add = jnp.dot(pick, back[b], preferred_element_type=jnp.float32)
            picked = add if picked is None else picked + add
        mixed = picked * weight if mixed is None else mixed + picked * weight
    mixed_ref[...] = mixed
    squares = to_row(jnp.sum(mixed * mixed, axis=1, keepdims=True), diag)
    squares_ref[...] = jnp.broadcast_to(squares[None], squares_ref.shape)


def norm_kernel(width, mixed_ref, squares_ref, gain_ref, out_ref):
    squares = jnp.sum(squares_ref[...], axis=0)[0:1, :]
    total = to_col(squares, eye(squares.shape[1]))
    scale = lax.rsqrt(total / width + epsilon)
    out_ref[...] = (mixed_ref[...] * scale * gain_ref[...]).astype(jnp.bfloat16)


CHUNKS = 8
PARTS = 4
WHOLE = pl.BlockSpec(memory_space=pltpu.VMEM)


def call(kernel, name, outs, *args, scratch=None):
    args = [pltpu.with_memory_space_constraint(a, pltpu.VMEM) for a in args]
    return pl.pallas_call(
        kernel,
        name=name,
        out_shape=outs,
        in_specs=[WHOLE] * len(args),
        out_specs=jax.tree.map(lambda _: WHOLE, outs, is_leaf=lambda o: hasattr(o, "dtype")),
        compiler_params=pltpu.CompilerParams(vmem_limit_bytes=16 << 20),
        scratch_shapes=[] if scratch is None else [pltpu.VMEM(scratch, jnp.float32)],
    )(*args)


def near(dims, dtype):
    return pltpu.VMEM(dims, dtype)


def per_device(tokens, pre_gain, post_gain, expert_ids, route_weights, w_gate, w_up, w_down):
    tok_rows, width = tokens.shape
    chips = lax.axis_size(CHIPS)
    tp = lax.axis_size("tp")
    slots = chips * CAP
    gate, up, down = w_gate[0], w_up[0], w_down[0]
    ff = gate.shape[1]
    cols = down.shape[1]
    flat = (slots * CHUNKS, 128)

    far = pl.BlockSpec(memory_space=pl.ANY)
    inputs = (tokens, pre_gain[None, :], expert_ids.T, route_weights.T, post_gain[None, :])
    buffer, place, mixing, post = pl.pallas_call(
        pre_kernel,
        name="pre",
        out_shape=(
            near(flat, jnp.bfloat16),
            near((2, tok_rows), jnp.float32),
            near((2, tok_rows), jnp.float32),
            near((1, cols), jnp.float32),
        ),
        in_specs=[far] * len(inputs),
        out_specs=(WHOLE,) * 4,
        compiler_params=pltpu.CompilerParams(vmem_limit_bytes=16 << 20),
        scratch_shapes=[
            pltpu.VMEM(flat, jnp.float32),
            pltpu.VMEM(tokens.shape, tokens.dtype),
            pltpu.VMEM(inputs[1].shape, jnp.float32),
            pltpu.VMEM(inputs[2].shape, jnp.int32),
            pltpu.SemaphoreType.DMA((PARTS + 4,)),
        ],
    )(*[pltpu.with_memory_space_constraint(a, pltpu.HBM) for a in inputs])

    def exchange(rows):
        pieces = rows.reshape(chips, CAP * CHUNKS, 128)
        return lax.all_to_all(pieces, CHIPS, 0, 0, tiled=True).reshape(flat)

    with jax.named_scope("dispatch"):
        arrived = exchange(buffer)

    first, second = weight_moves(tp)[0]
    with jax.named_scope("weights"):
        g1 = lax.ppermute(gate, ("ep_2", "tp"), first)
        u1 = lax.ppermute(up, ("ep_2", "tp"), first)
        g2 = lax.ppermute(gate, ("ep_2", "tp"), second)
        u2 = lax.ppermute(up, ("ep_2", "tp"), second)
        down_other = lax.ppermute(down, "ep_2", [(0, 1), (1, 0)])

    arrived, down_other = lax.optimization_barrier((arrived, down_other))
    with jax.named_scope("pair"):
        swaps = [(c * tp + t, c * tp + partner(c, t, tp)) for c in range(2) for t in range(tp)]
        theirs = lax.ppermute(arrived, ("ep_2", "tp"), swaps)
    weights = (gate, up, g1, u1, g2, u2)
    sums = call(
        first_kernel, "first", near((slots, 4 * ff), jnp.float32), arrived, *weights, scratch=flat
    )
    hidden = call(
        hidden_kernel,
        "hidden",
        near((tp, slots, 2 * ff), jnp.bfloat16),
        theirs,
        sums,
        *weights,
        scratch=flat,
    )
    with jax.named_scope("gather"):
        hidden = lax.all_to_all(hidden, "tp", 0, 0, tiled=True)
    results = call(
        down_kernel, "down", near(flat, jnp.bfloat16), hidden, down, down_other, scratch=flat
    )
    with jax.named_scope("back"):
        returned = exchange(results)
    mixed, squares = call(
        mix_kernel,
        "mix",
        (near((tok_rows, cols), jnp.float32), near((tp, 1, tok_rows), jnp.float32)),
        returned,
        place,
        mixing,
        scratch=flat,
    )
    with jax.named_scope("squares"):
        squares = lax.all_to_all(squares, "tp", 0, 0, tiled=True)
    return call(
        lambda *refs: norm_kernel(width, *refs),
        "norm",
        jax.ShapeDtypeStruct((tok_rows, cols), jnp.bfloat16),
        mixed,
        squares,
        post,
    )


def solution(mesh):
    torus = Mesh(mesh.devices.reshape(16, 4, 2, mesh.shape["tp"]), ("ep_0", "ep_1", "ep_2", "tp"))
    in_specs = (
        P(EP, None),
        P(),
        P("tp"),
        P(EP, None),
        P(EP, None),
        P(EP, None, "tp"),
        P(EP, None, "tp"),
        P(EP, None, "tp"),
    )
    return jax.shard_map(
        per_device, mesh=torus, in_specs=in_specs, out_specs=P(EP, "tp"), check_vma=False
    )
```

```python
import jax
import jax.numpy as jnp
from jax import lax
from jax.experimental import pallas as pl
from jax.experimental.pallas import tpu as pltpu
from jax.sharding import Mesh
from jax.sharding import PartitionSpec as P

EP = ("ep_0", "ep_1", "ep_2")
CHIPS = ("ep_0", "ep_1")
epsilon = 1e-06
CAP = 3


def eye(n):
    return lax.broadcasted_iota(jnp.int32, (n, n), 0) == lax.broadcasted_iota(jnp.int32, (n, n), 1)


def to_col(row, diag):
    return jnp.sum(jnp.where(diag, row, 0.0), axis=1, keepdims=True)


def to_row(col, diag):
    return jnp.sum(jnp.where(diag, col, 0.0), axis=0, keepdims=True)


def role(core, y):
    parity = jnp.where(core == 0, y // 2, (y + y // 2) % 2)
    half = jnp.where(core == 0, y % 2, y // 2)
    return parity, half


def partner(core, y, tp):
    return y ^ 1 if core == 0 else tp - 1 - y


def neighbour(core, y, tp):
    return partner(1 - core, y, tp)


def weight_moves(tp):
    edges = []
    for c in range(2):
        for y in range(tp):
            parity = y // 2 if c == 0 else (y + y // 2) % 2
            for n, s in enumerate((y, neighbour(c, y, tp))):
                if (parity, s) != (c, y):
                    edges.append(((parity, s), (c, y), n))
    color = {}

    def fits(i, r):
        return all(
            color[j] != r or (edges[j][0] != edges[i][0] and edges[j][1] != edges[i][1])
            for j in color
            if j != i
        )

    def place(i):
        if i == len(edges):
            return True
        for r in (1, 2):
            if fits(i, r):
                color[i] = r
                if place(i + 1):
                    return True
                del color[i]
        return False

    assert place(0)
    rounds = [[], []]
    comes = {(c, y): [0, 0] for c in range(2) for y in range(tp)}
    for i, (source, target, n) in enumerate(edges):
        rounds[color[i] - 1].append((source[0] * tp + source[1], target[0] * tp + target[1]))
        comes[target][n] = color[i]
    return rounds, comes


def spread(pieces_ref, scratch_ref):
    scratch_ref[...] = pieces_ref[...].astype(jnp.float32)
    return [chunk(scratch_ref, k)[...].astype(jnp.bfloat16) for k in range(CHUNKS)]


def chunk(scratch_ref, k):
    return scratch_ref.at[pl.ds(k, scratch_ref.shape[0] // CHUNKS, stride=CHUNKS), :]


def gathered(scratch_ref, out_ref):
    out_ref[...] = scratch_ref[...].astype(jnp.bfloat16)


def pre_kernel(
    tok_hbm,
    gain_hbm,
    ids_hbm,
    weight_hbm,
    post_hbm,
    gate_hbm,
    up_hbm,
    out_ref,
    place_ref,
    weight_ref,
    post_ref,
    both_ref,
    scratch_ref,
    tok_ref,
    gain_ref,
    ids_ref,
    sems,
):
    rows, width = tok_ref.shape
    half = CHUNKS * 128
    slots = out_ref.shape[0] // CHUNKS
    block = rows // PARTS
    pieces = [(ids_hbm, ids_ref)]
    for i in range(PARTS):
        span = pl.ds(i * block, block)
        pieces.append((tok_hbm.at[span, :], tok_ref.at[span, :]))
    pieces += [(gain_hbm, gain_ref), (weight_hbm, weight_ref), (post_hbm, post_ref)]
    pieces += [(gate_hbm, both_ref.at[0]), (up_hbm, both_ref.at[1])]
    copies = [pltpu.make_async_copy(a, b, sems.at[i]) for i, (a, b) in enumerate(pieces)]
    for copy in copies:
        copy.start()
    parity, side = role(lax.axis_index("ep_2"), lax.axis_index("tp"))
    parity = parity.astype(jnp.float32)
    start = pl.multiple_of(side * half, half)
    diag = eye(rows)
    lower = lax.broadcasted_iota(jnp.int32, (rows, rows), 0) < lax.broadcasted_iota(
        jnp.int32, (rows, rows), 1
    )
    copies[0].wait()
    ids = ids_ref[...].astype(jnp.float32)
    row0, row1 = ids[0:1, :], ids[1:2, :]
    col0, col1 = to_col(row0, diag), to_col(row1, diag)
    slot0 = jnp.sum(jnp.where((col0 == row0) & lower, 1.0, 0.0), axis=0, keepdims=True)
    slot1 = jnp.sum(jnp.where(col0 == row1, 1.0, 0.0), axis=0, keepdims=True) + jnp.sum(
        jnp.where((col1 == row1) & lower, 1.0, 0.0), axis=0, keepdims=True
    )
    chip0, chip1 = jnp.floor(row0 * 0.5), jnp.floor(row1 * 0.5)
    par0, par1 = row0 - 2.0 * chip0, row1 - 2.0 * chip1
    at0, at1 = CAP * chip0 + slot0, CAP * chip1 + slot1
    place_ref[0:1, :] = par0 * slots + at0
    place_ref[1:2, :] = par1 * slots + at1
    here0 = jnp.where(par0 == parity, at0, -1.0)
    here1 = jnp.where(par1 == parity, at1, -1.0)
    slot = lax.broadcasted_iota(jnp.int32, (slots, rows), 0).astype(jnp.float32)
    pick = jnp.where((slot == here0) | (slot == here1), 1.0, 0.0).astype(jnp.bfloat16)
    copies[PARTS + 1].wait()
    gain = gain_ref[:, pl.ds(start, half)]
    normed = []
    for i in range(PARTS):
        span = pl.ds(i * block, block)
        copies[1 + i].wait()
        values = tok_ref[span, :].astype(jnp.float32)
        scale = lax.rsqrt(jnp.mean(values * values, axis=1, keepdims=True) + epsilon)
        part = tok_ref[span, pl.ds(start, half)].astype(jnp.float32)
        normed.append((part * scale * gain).astype(jnp.bfloat16))
    normed = jnp.concatenate(normed, axis=0)
    sent = jnp.dot(pick, normed, preferred_element_type=jnp.float32)
    for k in range(CHUNKS):
        chunk(scratch_ref, k)[...] = sent[:, k * 128 : (k + 1) * 128]
    gathered(scratch_ref, out_ref)
    for copy in copies[PARTS + 2 :]:
        copy.wait()


def up_sums(pieces_ref, other, scratch_ref, weights, finish):
    half = CHUNKS * 128
    core, y = lax.axis_index("ep_2"), lax.axis_index("tp")
    side = role(core, y)[1]
    start = pl.multiple_of((1 - side if other else side) * half, half)
    rows = jnp.concatenate(spread(pieces_ref, scratch_ref), axis=1)

    def work(first, second):
        chosen = [(weights[r], i) for i in range(2) for r in (first, second)]
        columns = jnp.concatenate([w[i, pl.ds(start, half), :] for w, i in chosen], axis=1)
        finish(jnp.dot(rows, columns, preferred_element_type=jnp.float32))

    cases = {}
    for (c, t), comes in weight_moves(lax.axis_size("tp"))[1].items():
        cases.setdefault(tuple(comes), []).append((core == c) & (y == t))
    for comes, devices in sorted(cases.items()):
        here = devices[0]
        for device in devices[1:]:
            here = here | device
        pl.when(here)(lambda comes=comes: work(*comes))


def first_kernel(pieces_ref, w0, w1, w2, sums_ref, scratch_ref):
    def finish(sums):
        sums_ref[...] = sums

    up_sums(pieces_ref, False, scratch_ref, (w0, w1, w2), finish)


def hidden_kernel(pieces_ref, sums_ref, w0, w1, w2, out_ref, scratch_ref):
    def finish(sums):
        sums = sums_ref[...] + sums
        cols = out_ref.shape[2]
        gate, up = sums[:, :cols], sums[:, cols:]
        hidden = (gate / (1.0 + jnp.exp(-gate)) * up).astype(jnp.bfloat16)
        for i in range(out_ref.shape[0]):
            out_ref[i] = hidden

    up_sums(pieces_ref, True, scratch_ref, (w0, w1, w2), finish)


def down_kernel(hid_ref, mine_ref, other_ref, out_ref, scratch_ref):
    core = lax.axis_index("ep_2")
    slices = hid_ref.shape[0]
    wide = hid_ref.shape[2] // 2
    cols = mine_ref.shape[1]
    per = CHUNKS // 2

    def work(c, weights):
        for b, w in enumerate(weights):
            total = None
            for y in range(slices):
                if (y // 2 if c == 0 else (y + y // 2) % 2) != b:
                    continue
                for n, s in enumerate((y, neighbour(c, y, slices))):
                    add = jnp.dot(
                        hid_ref[y, :, n * wide : (n + 1) * wide],
                        w[s * wide : (s + 1) * wide, :],
                        preferred_element_type=jnp.float32,
                    )
                    total = add if total is None else total + add
            for k in range(per):
                chunk(scratch_ref, b * per + k)[...] = total[:, k * 128 : (k + 1) * 128]

    @pl.when(core == 0)
    def _():
        work(0, (mine_ref, other_ref))

    @pl.when(core == 1)
    def _():
        work(1, (other_ref, mine_ref))

    gathered(scratch_ref, out_ref)


def mix_kernel(back_ref, place_ref, weight_ref, mixed_ref, squares_ref, scratch_ref):
    slots = back_ref.shape[0] // CHUNKS
    rows, cols = mixed_ref.shape
    diag = eye(rows)
    lane = lax.broadcasted_iota(jnp.int32, (rows, slots), 1).astype(jnp.float32)
    pieces = spread(back_ref, scratch_ref)
    per = CHUNKS // 2
    back = [jnp.concatenate(pieces[b * per : (b + 1) * per], axis=1) for b in range(2)]
    mixed = None
    for k in range(2):
        place = to_col(place_ref[k : k + 1, :], diag)
        weight = to_col(weight_ref[k : k + 1, :], diag)
        picked = None
        for b in range(2):
            pick = jnp.where(lane + float(b * slots) == place, 1.0, 0.0).astype(jnp.bfloat16)
            add = jnp.dot(pick, back[b], preferred_element_type=jnp.float32)
            picked = add if picked is None else picked + add
        mixed = picked * weight if mixed is None else mixed + picked * weight
    mixed_ref[...] = mixed
    squares = to_row(jnp.sum(mixed * mixed, axis=1, keepdims=True), diag)
    squares_ref[...] = jnp.broadcast_to(squares[None], squares_ref.shape)


def norm_kernel(width, mixed_ref, squares_ref, gain_ref, out_ref):
    squares = jnp.sum(squares_ref[...], axis=0)[0:1, :]
    total = to_col(squares, eye(squares.shape[1]))
    scale = lax.rsqrt(total / width + epsilon)
    out_ref[...] = (mixed_ref[...] * scale * gain_ref[...]).astype(jnp.bfloat16)


CHUNKS = 8
PARTS = 4
WHOLE = pl.BlockSpec(memory_space=pltpu.VMEM)


def call(kernel, name, outs, *args, scratch=None):
    args = [pltpu.with_memory_space_constraint(a, pltpu.VMEM) for a in args]
    return pl.pallas_call(
        kernel,
        name=name,
        out_shape=outs,
        in_specs=[WHOLE] * len(args),
        out_specs=jax.tree.map(lambda _: WHOLE, outs, is_leaf=lambda o: hasattr(o, "dtype")),
        compiler_params=pltpu.CompilerParams(vmem_limit_bytes=16 << 20),
        scratch_shapes=[] if scratch is None else [pltpu.VMEM(scratch, jnp.float32)],
    )(*args)


def near(dims, dtype):
    return pltpu.VMEM(dims, dtype)


def per_device(tokens, pre_gain, post_gain, expert_ids, route_weights, w_gate, w_up, w_down):
    tok_rows, width = tokens.shape
    chips = lax.axis_size(CHIPS)
    tp = lax.axis_size("tp")
    slots = chips * CAP
    gate, up, down = w_gate[0], w_up[0], w_down[0]
    ff = gate.shape[1]
    cols = down.shape[1]
    flat = (slots * CHUNKS, 128)

    far = pl.BlockSpec(memory_space=pl.ANY)
    inputs = (
        tokens,
        pre_gain[None, :],
        expert_ids.T,
        route_weights.T,
        post_gain[None, :],
        gate,
        up,
    )
    buffer, place, mixing, post, both = pl.pallas_call(
        pre_kernel,
        name="pre",
        out_shape=(
            near(flat, jnp.bfloat16),
            near((2, tok_rows), jnp.float32),
            near((2, tok_rows), jnp.float32),
            near((1, cols), jnp.float32),
            near((2, *gate.shape), gate.dtype),
        ),
        in_specs=[far] * len(inputs),
        out_specs=(WHOLE,) * 5,
        compiler_params=pltpu.CompilerParams(vmem_limit_bytes=16 << 20),
        scratch_shapes=[
            pltpu.VMEM(flat, jnp.float32),
            pltpu.VMEM(tokens.shape, tokens.dtype),
            pltpu.VMEM(inputs[1].shape, jnp.float32),
            pltpu.VMEM(inputs[2].shape, jnp.int32),
            pltpu.SemaphoreType.DMA((PARTS + 6,)),
        ],
    )(*[pltpu.with_memory_space_constraint(a, pltpu.HBM) for a in inputs])

    def exchange(rows):
        pieces = rows.reshape(chips, CAP * CHUNKS, 128)
        return lax.all_to_all(pieces, CHIPS, 0, 0, tiled=True).reshape(flat)

    with jax.named_scope("dispatch"):
        arrived = exchange(buffer)

    first, second = weight_moves(tp)[0]
    with jax.named_scope("weights"):
        moved = [lax.ppermute(both, ("ep_2", "tp"), moves) for moves in (first, second)]
        down_other = lax.ppermute(down, "ep_2", [(0, 1), (1, 0)])

    arrived, down_other = lax.optimization_barrier((arrived, down_other))
    with jax.named_scope("pair"):
        swaps = [(c * tp + t, c * tp + partner(c, t, tp)) for c in range(2) for t in range(tp)]
        theirs = lax.ppermute(arrived, ("ep_2", "tp"), swaps)
    weights = (both, *moved)
    sums = call(
        first_kernel, "first", near((slots, 4 * ff), jnp.float32), arrived, *weights, scratch=flat
    )
    hidden = call(
        hidden_kernel,
        "hidden",
        near((tp, slots, 2 * ff), jnp.bfloat16),
        theirs,
        sums,
        *weights,
        scratch=flat,
    )
    with jax.named_scope("gather"):
        hidden = lax.all_to_all(hidden, "tp", 0, 0, tiled=True)
    results = call(
        down_kernel, "down", near(flat, jnp.bfloat16), hidden, down, down_other, scratch=flat
    )
    with jax.named_scope("back"):
        returned = exchange(results)
    mixed, squares = call(
        mix_kernel,
        "mix",
        (near((tok_rows, cols), jnp.float32), near((tp, 1, tok_rows), jnp.float32)),
        returned,
        place,
        mixing,
        scratch=flat,
    )
    with jax.named_scope("squares"):
        squares = lax.all_to_all(squares, "tp", 0, 0, tiled=True)
    return call(
        lambda *refs: norm_kernel(width, *refs),
        "norm",
        jax.ShapeDtypeStruct((tok_rows, cols), jnp.bfloat16),
        mixed,
        squares,
        post,
    )


def solution(mesh):
    torus = Mesh(mesh.devices.reshape(16, 4, 2, mesh.shape["tp"]), ("ep_0", "ep_1", "ep_2", "tp"))
    in_specs = (
        P(EP, None),
        P(),
        P("tp"),
        P(EP, None),
        P(EP, None),
        P(EP, None, "tp"),
        P(EP, None, "tp"),
        P(EP, None, "tp"),
    )
    return jax.shard_map(
        per_device, mesh=torus, in_specs=in_specs, out_specs=P(EP, "tp"), check_vma=False
    )
```

```python
import jax
import jax.numpy as jnp
from jax import lax
from jax.experimental import pallas as pl
from jax.experimental.pallas import tpu as pltpu
from jax.sharding import Mesh
from jax.sharding import PartitionSpec as P

EP = ("ep_0", "ep_1", "ep_2")
CHIPS = ("ep_0", "ep_1")
epsilon = 1e-06
CAP = 3


def eye(n):
    return lax.broadcasted_iota(jnp.int32, (n, n), 0) == lax.broadcasted_iota(jnp.int32, (n, n), 1)


def to_col(row, diag):
    return jnp.sum(jnp.where(diag, row, 0.0), axis=1, keepdims=True)


def to_row(col, diag):
    return jnp.sum(jnp.where(diag, col, 0.0), axis=0, keepdims=True)


def role(core, y):
    parity = jnp.where(core == 0, y // 2, (y + y // 2) % 2)
    half = jnp.where(core == 0, y % 2, y // 2)
    return parity, half


def partner(core, y, tp):
    return y ^ 1 if core == 0 else tp - 1 - y


def neighbour(core, y, tp):
    return partner(1 - core, y, tp)


def weight_moves(tp):
    edges = []
    for c in range(2):
        for y in range(tp):
            parity = y // 2 if c == 0 else (y + y // 2) % 2
            for n, s in enumerate((y, neighbour(c, y, tp))):
                if (parity, s) != (c, y):
                    edges.append(((parity, s), (c, y), n))
    color = {}

    def fits(i, r):
        return all(
            color[j] != r or (edges[j][0] != edges[i][0] and edges[j][1] != edges[i][1])
            for j in color
            if j != i
        )

    def place(i):
        if i == len(edges):
            return True
        for r in (1, 2):
            if fits(i, r):
                color[i] = r
                if place(i + 1):
                    return True
                del color[i]
        return False

    assert place(0)
    rounds = [[], []]
    comes = {(c, y): [0, 0] for c in range(2) for y in range(tp)}
    for i, (source, target, n) in enumerate(edges):
        rounds[color[i] - 1].append((source[0] * tp + source[1], target[0] * tp + target[1]))
        comes[target][n] = color[i]
    return rounds, comes


def spread(pieces_ref, scratch_ref):
    scratch_ref[...] = pieces_ref[...].astype(jnp.float32)
    return [chunk(scratch_ref, k)[...].astype(jnp.bfloat16) for k in range(CHUNKS)]


def chunk(scratch_ref, k):
    return scratch_ref.at[pl.ds(k, scratch_ref.shape[0] // CHUNKS, stride=CHUNKS), :]


def gathered(scratch_ref, out_ref):
    out_ref[...] = scratch_ref[...].astype(jnp.bfloat16)


def seat(chip, chips):
    place = chip + float(chips - FIRST % chips)
    return jnp.where(place < chips, place, place - chips)


def pre_kernel(
    tok_hbm,
    gain_hbm,
    ids_hbm,
    weight_hbm,
    post_hbm,
    gate_hbm,
    up_hbm,
    out_ref,
    place_ref,
    weight_ref,
    post_ref,
    both_ref,
    scratch_ref,
    tok_ref,
    gain_ref,
    ids_ref,
    sems,
):
    rows, width = tok_ref.shape
    half = CHUNKS * 128
    slots = out_ref.shape[0] // CHUNKS
    chips = slots // CAP
    block = rows // PARTS
    pieces = [(ids_hbm, ids_ref)]
    for i in range(PARTS):
        span = pl.ds(i * block, block)
        pieces.append((tok_hbm.at[span, :], tok_ref.at[span, :]))
    pieces += [(gain_hbm, gain_ref), (weight_hbm, weight_ref), (post_hbm, post_ref)]
    pieces += [(gate_hbm, both_ref.at[0]), (up_hbm, both_ref.at[1])]
    copies = [pltpu.make_async_copy(a, b, sems.at[i]) for i, (a, b) in enumerate(pieces)]
    for copy in copies:
        copy.start()
    parity, side = role(lax.axis_index("ep_2"), lax.axis_index("tp"))
    parity = parity.astype(jnp.float32)
    start = pl.multiple_of(side * half, half)
    diag = eye(rows)
    lower = lax.broadcasted_iota(jnp.int32, (rows, rows), 0) < lax.broadcasted_iota(
        jnp.int32, (rows, rows), 1
    )
    copies[0].wait()
    ids = ids_ref[...].astype(jnp.float32)
    row0, row1 = ids[0:1, :], ids[1:2, :]
    col0, col1 = to_col(row0, diag), to_col(row1, diag)
    slot0 = jnp.sum(jnp.where((col0 == row0) & lower, 1.0, 0.0), axis=0, keepdims=True)
    slot1 = jnp.sum(jnp.where(col0 == row1, 1.0, 0.0), axis=0, keepdims=True) + jnp.sum(
        jnp.where((col1 == row1) & lower, 1.0, 0.0), axis=0, keepdims=True
    )
    chip0, chip1 = jnp.floor(row0 * 0.5), jnp.floor(row1 * 0.5)
    par0, par1 = row0 - 2.0 * chip0, row1 - 2.0 * chip1
    at0, at1 = CAP * seat(chip0, chips) + slot0, CAP * seat(chip1, chips) + slot1
    place_ref[0:1, :] = par0 * slots + at0
    place_ref[1:2, :] = par1 * slots + at1
    here0 = jnp.where(par0 == parity, at0, -1.0)
    here1 = jnp.where(par1 == parity, at1, -1.0)
    slot = lax.broadcasted_iota(jnp.int32, (slots, rows), 0).astype(jnp.float32)
    pick = jnp.where((slot == here0) | (slot == here1), 1.0, 0.0).astype(jnp.bfloat16)
    copies[PARTS + 1].wait()
    gain = gain_ref[:, pl.ds(start, half)]
    normed = []
    for i in range(PARTS):
        span = pl.ds(i * block, block)
        copies[1 + i].wait()
        values = tok_ref[span, :].astype(jnp.float32)
        scale = lax.rsqrt(jnp.mean(values * values, axis=1, keepdims=True) + epsilon)
        part = tok_ref[span, pl.ds(start, half)].astype(jnp.float32)
        normed.append((part * scale * gain).astype(jnp.bfloat16))
    normed = jnp.concatenate(normed, axis=0)
    sent = jnp.dot(pick, normed, preferred_element_type=jnp.float32)
    for k in range(CHUNKS):
        chunk(scratch_ref, k)[...] = sent[:, k * 128 : (k + 1) * 128]
    gathered(scratch_ref, out_ref)
    for copy in copies[PARTS + 2 :]:
        copy.wait()


def up_sums(pieces_ref, other, scratch_ref, weights, finish):
    half = CHUNKS * 128
    core, y = lax.axis_index("ep_2"), lax.axis_index("tp")
    side = role(core, y)[1]
    start = pl.multiple_of((1 - side if other else side) * half, half)
    rows = jnp.concatenate(spread(pieces_ref, scratch_ref), axis=1)

    def work(first, second):
        chosen = [(weights[r], i) for i in range(2) for r in (first, second)]
        columns = jnp.concatenate([w[i, pl.ds(start, half), :] for w, i in chosen], axis=1)
        finish(jnp.dot(rows, columns, preferred_element_type=jnp.float32))

    cases = {}
    for (c, t), comes in weight_moves(lax.axis_size("tp"))[1].items():
        cases.setdefault(tuple(comes), []).append((core == c) & (y == t))
    for comes, devices in sorted(cases.items()):
        here = devices[0]
        for device in devices[1:]:
            here = here | device
        pl.when(here)(lambda comes=comes: work(*comes))


def first_kernel(pieces_ref, w0, w1, w2, sums_ref, scratch_ref):
    def finish(sums):
        sums_ref[...] = sums

    up_sums(pieces_ref, False, scratch_ref, (w0, w1, w2), finish)


def hidden_kernel(pieces_ref, sums_ref, w0, w1, w2, out_ref, scratch_ref):
    def finish(sums):
        sums = sums_ref[...] + sums
        cols = out_ref.shape[2]
        gate, up = sums[:, :cols], sums[:, cols:]
        hidden = (gate / (1.0 + jnp.exp(-gate)) * up).astype(jnp.bfloat16)
        for i in range(out_ref.shape[0]):
            out_ref[i] = hidden

    up_sums(pieces_ref, True, scratch_ref, (w0, w1, w2), finish)


def down_kernel(hid_ref, mine_ref, other_ref, out_ref, scratch_ref):
    core = lax.axis_index("ep_2")
    slices = hid_ref.shape[0]
    wide = hid_ref.shape[2] // 2
    cols = mine_ref.shape[1]
    per = CHUNKS // 2

    def work(c, weights):
        for b, w in enumerate(weights):
            total = None
            for y in range(slices):
                if (y // 2 if c == 0 else (y + y // 2) % 2) != b:
                    continue
                for n, s in enumerate((y, neighbour(c, y, slices))):
                    add = jnp.dot(
                        hid_ref[y, :, n * wide : (n + 1) * wide],
                        w[s * wide : (s + 1) * wide, :],
                        preferred_element_type=jnp.float32,
                    )
                    total = add if total is None else total + add
            for k in range(per):
                chunk(scratch_ref, b * per + k)[...] = total[:, k * 128 : (k + 1) * 128]

    @pl.when(core == 0)
    def _():
        work(0, (mine_ref, other_ref))

    @pl.when(core == 1)
    def _():
        work(1, (other_ref, mine_ref))

    gathered(scratch_ref, out_ref)


def mix_kernel(back_ref, place_ref, weight_ref, mixed_ref, squares_ref, scratch_ref):
    slots = back_ref.shape[0] // CHUNKS
    rows, cols = mixed_ref.shape
    diag = eye(rows)
    lane = lax.broadcasted_iota(jnp.int32, (rows, slots), 1).astype(jnp.float32)
    pieces = spread(back_ref, scratch_ref)
    per = CHUNKS // 2
    back = [jnp.concatenate(pieces[b * per : (b + 1) * per], axis=1) for b in range(2)]
    mixed = None
    for k in range(2):
        place = to_col(place_ref[k : k + 1, :], diag)
        weight = to_col(weight_ref[k : k + 1, :], diag)
        picked = None
        for b in range(2):
            pick = jnp.where(lane + float(b * slots) == place, 1.0, 0.0).astype(jnp.bfloat16)
            add = jnp.dot(pick, back[b], preferred_element_type=jnp.float32)
            picked = add if picked is None else picked + add
        mixed = picked * weight if mixed is None else mixed + picked * weight
    mixed_ref[...] = mixed
    squares = to_row(jnp.sum(mixed * mixed, axis=1, keepdims=True), diag)
    squares_ref[...] = jnp.broadcast_to(squares[None], squares_ref.shape)


def norm_kernel(width, mixed_ref, squares_ref, gain_ref, out_ref):
    squares = jnp.sum(squares_ref[...], axis=0)[0:1, :]
    total = to_col(squares, eye(squares.shape[1]))
    scale = lax.rsqrt(total / width + epsilon)
    out_ref[...] = (mixed_ref[...] * scale * gain_ref[...]).astype(jnp.bfloat16)


CHUNKS = 8
PARTS = 2
FIRST = 40
WHOLE = pl.BlockSpec(memory_space=pltpu.VMEM)


def call(kernel, name, outs, *args, scratch=None):
    args = [pltpu.with_memory_space_constraint(a, pltpu.VMEM) for a in args]
    return pl.pallas_call(
        kernel,
        name=name,
        out_shape=outs,
        in_specs=[WHOLE] * len(args),
        out_specs=jax.tree.map(lambda _: WHOLE, outs, is_leaf=lambda o: hasattr(o, "dtype")),
        compiler_params=pltpu.CompilerParams(vmem_limit_bytes=16 << 20),
        scratch_shapes=[] if scratch is None else [pltpu.VMEM(scratch, jnp.float32)],
    )(*args)


def near(dims, dtype):
    return pltpu.VMEM(dims, dtype)


def per_device(tokens, pre_gain, post_gain, expert_ids, route_weights, w_gate, w_up, w_down):
    tok_rows, width = tokens.shape
    chips = lax.axis_size(CHIPS)
    tp = lax.axis_size("tp")
    slots = chips * CAP
    gate, up, down = w_gate[0], w_up[0], w_down[0]
    ff = gate.shape[1]
    cols = down.shape[1]
    flat = (slots * CHUNKS, 128)

    far = pl.BlockSpec(memory_space=pl.ANY)
    inputs = (
        tokens,
        pre_gain[None, :],
        expert_ids.T,
        route_weights.T,
        post_gain[None, :],
        gate,
        up,
    )
    buffer, place, mixing, post, both = pl.pallas_call(
        pre_kernel,
        name="pre",
        out_shape=(
            near(flat, jnp.bfloat16),
            near((2, tok_rows), jnp.float32),
            near((2, tok_rows), jnp.float32),
            near((1, cols), jnp.float32),
            near((2, *gate.shape), gate.dtype),
        ),
        in_specs=[far] * len(inputs),
        out_specs=(WHOLE,) * 5,
        compiler_params=pltpu.CompilerParams(vmem_limit_bytes=16 << 20),
        scratch_shapes=[
            pltpu.VMEM(flat, jnp.float32),
            pltpu.VMEM(tokens.shape, tokens.dtype),
            pltpu.VMEM(inputs[1].shape, jnp.float32),
            pltpu.VMEM(inputs[2].shape, jnp.int32),
            pltpu.SemaphoreType.DMA((PARTS + 6,)),
        ],
    )(*[pltpu.with_memory_space_constraint(a, pltpu.HBM) for a in inputs])

    def exchange(rows):
        pieces = rows.reshape(chips, CAP * CHUNKS, 128)
        groups = [[(p + FIRST) % chips * 2 + c for p in range(chips)] for c in range(2)]
        return lax.all_to_all(
            pieces, EP, 0, 0, tiled=True, axis_index_groups=groups
        ).reshape(flat)

    with jax.named_scope("dispatch"):
        arrived = exchange(buffer)

    first, second = weight_moves(tp)[0]
    with jax.named_scope("weights"):
        moved = [lax.ppermute(both, ("ep_2", "tp"), moves) for moves in (first, second)]
        down_other = lax.ppermute(down, "ep_2", [(0, 1), (1, 0)])

    arrived, down_other = lax.optimization_barrier((arrived, down_other))
    with jax.named_scope("pair"):
        swaps = [(c * tp + t, c * tp + partner(c, t, tp)) for c in range(2) for t in range(tp)]
        theirs = lax.ppermute(arrived, ("ep_2", "tp"), swaps)
    weights = (both, *moved)
    sums = call(
        first_kernel, "first", near((slots, 4 * ff), jnp.float32), arrived, *weights, scratch=flat
    )
    hidden = call(
        hidden_kernel,
        "hidden",
        near((tp, slots, 2 * ff), jnp.bfloat16),
        theirs,
        sums,
        *weights,
        scratch=flat,
    )
    with jax.named_scope("gather"):
        hidden = lax.all_to_all(hidden, "tp", 0, 0, tiled=True)
    results = call(
        down_kernel, "down", near(flat, jnp.bfloat16), hidden, down, down_other, scratch=flat
    )
    with jax.named_scope("back"):
        returned = exchange(results)
    mixed, squares = call(
        mix_kernel,
        "mix",
        (near((tok_rows, cols), jnp.float32), near((tp, 1, tok_rows), jnp.float32)),
        returned,
        place,
        mixing,
        scratch=flat,
    )
    with jax.named_scope("squares"):
        squares = lax.all_to_all(squares, "tp", 0, 0, tiled=True)
    return call(
        lambda *refs: norm_kernel(width, *refs),
        "norm",
        jax.ShapeDtypeStruct((tok_rows, cols), jnp.bfloat16),
        mixed,
        squares,
        post,
    )


def solution(mesh):
    torus = Mesh(mesh.devices.reshape(16, 4, 2, mesh.shape["tp"]), ("ep_0", "ep_1", "ep_2", "tp"))
    in_specs = (
        P(EP, None),
        P(),
        P("tp"),
        P(EP, None),
        P(EP, None),
        P(EP, None, "tp"),
        P(EP, None, "tp"),
        P(EP, None, "tp"),
    )
    return jax.shard_map(
        per_device, mesh=torus, in_specs=in_specs, out_specs=P(EP, "tp"), check_vma=False
    )
```

```python
import jax
import jax.numpy as jnp
from jax import lax
from jax.experimental import pallas as pl
from jax.experimental.pallas import tpu as pltpu
from jax.sharding import Mesh
from jax.sharding import PartitionSpec as P

EP = ("ep_0", "ep_1", "ep_2")
CHIPS = ("ep_0", "ep_1")
epsilon = 1e-06
CAP = 3


def eye(n):
    return lax.broadcasted_iota(jnp.int32, (n, n), 0) == lax.broadcasted_iota(jnp.int32, (n, n), 1)


def to_col(row, diag):
    return jnp.sum(jnp.where(diag, row, 0.0), axis=1, keepdims=True)


def to_row(col, diag):
    return jnp.sum(jnp.where(diag, col, 0.0), axis=0, keepdims=True)


def role(core, y):
    parity = jnp.where(core == 0, y // 2, (y + y // 2) % 2)
    half = jnp.where(core == 0, y % 2, y // 2)
    return parity, half


def partner(core, y, tp):
    return y ^ 1 if core == 0 else tp - 1 - y


def neighbour(core, y, tp):
    return partner(1 - core, y, tp)


def weight_moves(tp):
    edges = []
    for c in range(2):
        for y in range(tp):
            parity = y // 2 if c == 0 else (y + y // 2) % 2
            for n, s in enumerate((y, neighbour(c, y, tp))):
                if (parity, s) != (c, y):
                    edges.append(((parity, s), (c, y), n))
    color = {}

    def fits(i, r):
        return all(
            color[j] != r or (edges[j][0] != edges[i][0] and edges[j][1] != edges[i][1])
            for j in color
            if j != i
        )

    def place(i):
        if i == len(edges):
            return True
        for r in (1, 2):
            if fits(i, r):
                color[i] = r
                if place(i + 1):
                    return True
                del color[i]
        return False

    assert place(0)
    rounds = [[], []]
    comes = {(c, y): [0, 0] for c in range(2) for y in range(tp)}
    for i, (source, target, n) in enumerate(edges):
        rounds[color[i] - 1].append((source[0] * tp + source[1], target[0] * tp + target[1]))
        comes[target][n] = color[i]
    return rounds, comes


def spread(pieces_ref, scratch_ref):
    scratch_ref[...] = pieces_ref[...].astype(jnp.float32)
    return [chunk(scratch_ref, k)[...].astype(jnp.bfloat16) for k in range(CHUNKS)]


def chunk(scratch_ref, k):
    return scratch_ref.at[pl.ds(k, scratch_ref.shape[0] // CHUNKS, stride=CHUNKS), :]


def gathered(scratch_ref, out_ref):
    out_ref[...] = scratch_ref[...].astype(jnp.bfloat16)


def seat(chip, chips):
    place = chip + float(chips - FIRST % chips)
    return jnp.where(place < chips, place, place - chips)


def pre_kernel(
    tok_hbm,
    gain_hbm,
    ids_hbm,
    weight_hbm,
    post_hbm,
    gate_hbm,
    up_hbm,
    out_ref,
    place_ref,
    weight_ref,
    post_ref,
    both_ref,
    scratch_ref,
    tok_ref,
    gain_ref,
    ids_ref,
    sems,
):
    rows, width = tok_ref.shape
    half = CHUNKS * 128
    slots = out_ref.shape[0] // CHUNKS
    chips = slots // CAP
    block = rows // PARTS
    pieces = [(ids_hbm, ids_ref)]
    for i in range(PARTS):
        span = pl.ds(i * block, block)
        pieces.append((tok_hbm.at[span, :], tok_ref.at[span, :]))
    pieces += [(gain_hbm, gain_ref), (weight_hbm, weight_ref), (post_hbm, post_ref)]
    pieces += [(gate_hbm, both_ref.at[0]), (up_hbm, both_ref.at[1])]
    copies = [pltpu.make_async_copy(a, b, sems.at[i]) for i, (a, b) in enumerate(pieces)]
    for copy in copies:
        copy.start()
    parity, side = role(lax.axis_index("ep_2"), lax.axis_index("tp"))
    parity = parity.astype(jnp.float32)
    start = pl.multiple_of(side * half, half)
    diag = eye(rows)
    lower = lax.broadcasted_iota(jnp.int32, (rows, rows), 0) < lax.broadcasted_iota(
        jnp.int32, (rows, rows), 1
    )
    copies[0].wait()
    ids = ids_ref[...].astype(jnp.float32)
    row0, row1 = ids[0:1, :], ids[1:2, :]
    col0, col1 = to_col(row0, diag), to_col(row1, diag)
    slot0 = jnp.sum(jnp.where((col0 == row0) & lower, 1.0, 0.0), axis=0, keepdims=True)
    slot1 = jnp.sum(jnp.where(col0 == row1, 1.0, 0.0), axis=0, keepdims=True) + jnp.sum(
        jnp.where((col1 == row1) & lower, 1.0, 0.0), axis=0, keepdims=True
    )
    chip0, chip1 = jnp.floor(row0 * 0.5), jnp.floor(row1 * 0.5)
    par0, par1 = row0 - 2.0 * chip0, row1 - 2.0 * chip1
    at0, at1 = CAP * seat(chip0, chips) + slot0, CAP * seat(chip1, chips) + slot1
    place_ref[0:1, :] = par0 * slots + at0
    place_ref[1:2, :] = par1 * slots + at1
    here0 = jnp.where(par0 == parity, at0, -1.0)
    here1 = jnp.where(par1 == parity, at1, -1.0)
    slot = lax.broadcasted_iota(jnp.int32, (slots, rows), 0).astype(jnp.float32)
    pick = jnp.where((slot == here0) | (slot == here1), 1.0, 0.0).astype(jnp.bfloat16)
    copies[PARTS + 1].wait()
    gain = gain_ref[:, pl.ds(start, half)]
    normed = []
    for i in range(PARTS):
        span = pl.ds(i * block, block)
        copies[1 + i].wait()
        values = tok_ref[span, :].astype(jnp.float32)
        scale = lax.rsqrt(jnp.mean(values * values, axis=1, keepdims=True) + epsilon)
        part = tok_ref[span, pl.ds(start, half)].astype(jnp.float32)
        normed.append((part * scale * gain).astype(jnp.bfloat16))
    normed = jnp.concatenate(normed, axis=0)
    sent = jnp.dot(pick, normed, preferred_element_type=jnp.float32)
    for k in range(CHUNKS):
        chunk(scratch_ref, k)[...] = sent[:, k * 128 : (k + 1) * 128]
    gathered(scratch_ref, out_ref)
    for copy in copies[PARTS + 2 :]:
        copy.wait()


def up_sums(pieces_ref, other, scratch_ref, weights, finish):
    half = CHUNKS * 128
    core, y = lax.axis_index("ep_2"), lax.axis_index("tp")
    side = role(core, y)[1]
    start = pl.multiple_of((1 - side if other else side) * half, half)
    rows = jnp.concatenate(spread(pieces_ref, scratch_ref), axis=1)

    def work(first, second):
        chosen = [(weights[r], i) for i in range(2) for r in (first, second)]
        columns = jnp.concatenate([w[i, pl.ds(start, half), :] for w, i in chosen], axis=1)
        finish(jnp.dot(rows, columns, preferred_element_type=jnp.float32))

    cases = {}
    for (c, t), comes in weight_moves(lax.axis_size("tp"))[1].items():
        cases.setdefault(tuple(comes), []).append((core == c) & (y == t))
    for comes, devices in sorted(cases.items()):
        here = devices[0]
        for device in devices[1:]:
            here = here | device
        pl.when(here)(lambda comes=comes: work(*comes))


def first_kernel(pieces_ref, w0, w1, w2, sums_ref, scratch_ref):
    def finish(sums):
        sums_ref[...] = sums

    up_sums(pieces_ref, False, scratch_ref, (w0, w1, w2), finish)


def hidden_kernel(pieces_ref, sums_ref, w0, w1, w2, out_ref, scratch_ref):
    def finish(sums):
        sums = sums_ref[...] + sums
        cols = out_ref.shape[2]
        gate, up = sums[:, :cols], sums[:, cols:]
        hidden = (gate / (1.0 + jnp.exp(-gate)) * up).astype(jnp.bfloat16)
        for i in range(out_ref.shape[0]):
            out_ref[i] = hidden

    up_sums(pieces_ref, True, scratch_ref, (w0, w1, w2), finish)


def down_kernel(hid_ref, mine_ref, other_ref, out_ref, scratch_ref):
    core = lax.axis_index("ep_2")
    slices = hid_ref.shape[0]
    wide = hid_ref.shape[2] // 2
    cols = mine_ref.shape[1]
    per = CHUNKS // 2

    def work(c, weights):
        for b, w in enumerate(weights):
            total = None
            for y in range(slices):
                if (y // 2 if c == 0 else (y + y // 2) % 2) != b:
                    continue
                for n, s in enumerate((y, neighbour(c, y, slices))):
                    add = jnp.dot(
                        hid_ref[y, :, n * wide : (n + 1) * wide],
                        w[s * wide : (s + 1) * wide, :],
                        preferred_element_type=jnp.float32,
                    )
                    total = add if total is None else total + add
            for k in range(per):
                chunk(scratch_ref, b * per + k)[...] = total[:, k * 128 : (k + 1) * 128]

    @pl.when(core == 0)
    def _():
        work(0, (mine_ref, other_ref))

    @pl.when(core == 1)
    def _():
        work(1, (other_ref, mine_ref))

    gathered(scratch_ref, out_ref)


def mix_kernel(back_ref, place_ref, weight_ref, mixed_ref, squares_ref, scratch_ref):
    slots = back_ref.shape[0] // CHUNKS
    rows, cols = mixed_ref.shape
    diag = eye(rows)
    lane = lax.broadcasted_iota(jnp.int32, (rows, slots), 1).astype(jnp.float32)
    pieces = spread(back_ref, scratch_ref)
    per = CHUNKS // 2
    back = [jnp.concatenate(pieces[b * per : (b + 1) * per], axis=1) for b in range(2)]
    mixed = None
    for k in range(2):
        place = to_col(place_ref[k : k + 1, :], diag)
        weight = to_col(weight_ref[k : k + 1, :], diag)
        picked = None
        for b in range(2):
            pick = jnp.where(lane + float(b * slots) == place, 1.0, 0.0).astype(jnp.bfloat16)
            add = jnp.dot(pick, back[b], preferred_element_type=jnp.float32)
            picked = add if picked is None else picked + add
        mixed = picked * weight if mixed is None else mixed + picked * weight
    mixed_ref[...] = mixed
    squares = to_row(jnp.sum(mixed * mixed, axis=1, keepdims=True), diag)
    squares_ref[...] = jnp.broadcast_to(squares[None], squares_ref.shape)


def norm_kernel(width, mixed_ref, squares_ref, gain_ref, out_ref):
    squares = jnp.sum(squares_ref[...], axis=0)[0:1, :]
    total = to_col(squares, eye(squares.shape[1]))
    scale = lax.rsqrt(total / width + epsilon)
    out_ref[...] = (mixed_ref[...] * scale * gain_ref[...]).astype(jnp.bfloat16)


CHUNKS = 8
PARTS = 2
FIRST = 40
WHOLE = pl.BlockSpec(memory_space=pltpu.VMEM)


def call(kernel, name, outs, *args, scratch=None):
    args = [pltpu.with_memory_space_constraint(a, pltpu.VMEM) for a in args]
    return pl.pallas_call(
        kernel,
        name=name,
        out_shape=outs,
        in_specs=[WHOLE] * len(args),
        out_specs=jax.tree.map(lambda _: WHOLE, outs, is_leaf=lambda o: hasattr(o, "dtype")),
        compiler_params=pltpu.CompilerParams(vmem_limit_bytes=16 << 20),
        scratch_shapes=[] if scratch is None else [pltpu.VMEM(scratch, jnp.float32)],
    )(*args)


def near(dims, dtype):
    return pltpu.VMEM(dims, dtype)


def per_device(tokens, pre_gain, post_gain, expert_ids, route_weights, w_gate, w_up, w_down):
    tok_rows, width = tokens.shape
    chips = lax.axis_size(CHIPS)
    tp = lax.axis_size("tp")
    slots = chips * CAP
    gate, up, down = w_gate[0], w_up[0], w_down[0]
    ff = gate.shape[1]
    cols = down.shape[1]
    flat = (slots * CHUNKS, 128)

    far = pl.BlockSpec(memory_space=pl.ANY)
    inputs = (
        tokens,
        pre_gain[None, :],
        expert_ids.T,
        route_weights.T,
        post_gain[None, :],
        gate,
        up,
    )
    buffer, place, mixing, post, both = pl.pallas_call(
        pre_kernel,
        name="pre",
        out_shape=(
            near(flat, jnp.bfloat16),
            near((2, tok_rows), jnp.float32),
            near((2, tok_rows), jnp.float32),
            near((1, cols), jnp.float32),
            near((2, *gate.shape), gate.dtype),
        ),
        in_specs=[far] * len(inputs),
        out_specs=(WHOLE,) * 5,
        compiler_params=pltpu.CompilerParams(vmem_limit_bytes=16 << 20),
        scratch_shapes=[
            pltpu.VMEM(flat, jnp.float32),
            pltpu.VMEM(tokens.shape, tokens.dtype),
            pltpu.VMEM(inputs[1].shape, jnp.float32),
            pltpu.VMEM(inputs[2].shape, jnp.int32),
            pltpu.SemaphoreType.DMA((PARTS + 6,)),
        ],
    )(*[pltpu.with_memory_space_constraint(a, pltpu.HBM) for a in inputs])

    def exchange(rows):
        pieces = rows.reshape(chips, CAP * CHUNKS, 128)
        groups = [[(p + FIRST) % chips * 2 + c for p in range(chips)] for c in range(2)]
        return lax.all_to_all(
            pieces, EP, 0, 0, tiled=True, axis_index_groups=groups
        ).reshape(flat)

    with jax.named_scope("dispatch"):
        arrived = exchange(buffer)

    first, second = weight_moves(tp)[0]
    with jax.named_scope("weights"):
        moved = [lax.ppermute(both, ("ep_2", "tp"), moves) for moves in (first, second)]
        down_other = lax.ppermute(down, "ep_2", [(0, 1), (1, 0)])

    arrived, down_other = lax.optimization_barrier((arrived, down_other))
    with jax.named_scope("pair"):
        swaps = [(c * tp + t, c * tp + partner(c, t, tp)) for c in range(2) for t in range(tp)]
        theirs = lax.ppermute(arrived, ("ep_2", "tp"), swaps)
    weights = (both, *moved)
    sums = call(
        first_kernel, "first", near((slots, 4 * ff), jnp.float32), arrived, *weights, scratch=flat
    )
    hidden = call(
        hidden_kernel,
        "hidden",
        near((tp, slots, 2 * ff), jnp.bfloat16),
        theirs,
        sums,
        *weights,
        scratch=flat,
    )
    with jax.named_scope("gather"):
        hidden = lax.all_to_all(hidden, "tp", 0, 0, tiled=True)
    results = call(
        down_kernel, "down", near(flat, jnp.bfloat16), hidden, down, down_other, scratch=flat
    )
    with jax.named_scope("back"):
        returned = exchange(results)
    mixed, squares = call(
        mix_kernel,
        "mix",
        (near((tok_rows, cols), jnp.float32), near((tp, 1, tok_rows), jnp.float32)),
        returned,
        place,
        mixing,
        scratch=flat,
    )
    with jax.named_scope("squares"):
        squares = lax.all_to_all(squares, "tp", 0, 0, tiled=True, axis_index_groups=[[2, 3, 0, 1]])
    return call(
        lambda *refs: norm_kernel(width, *refs),
        "norm",
        jax.ShapeDtypeStruct((tok_rows, cols), jnp.bfloat16),
        mixed,
        squares,
        post,
    )


def solution(mesh):
    torus = Mesh(mesh.devices.reshape(16, 4, 2, mesh.shape["tp"]), ("ep_0", "ep_1", "ep_2", "tp"))
    in_specs = (
        P(EP, None),
        P(),
        P("tp"),
        P(EP, None),
        P(EP, None),
        P(EP, None, "tp"),
        P(EP, None, "tp"),
        P(EP, None, "tp"),
    )
    return jax.shard_map(
        per_device, mesh=torus, in_specs=in_specs, out_specs=P(EP, "tp"), check_vma=False
    )
```

```python
import jax
import jax.numpy as jnp
from jax import lax
from jax.experimental import pallas as pl
from jax.experimental.pallas import tpu as pltpu
from jax.sharding import Mesh
from jax.sharding import PartitionSpec as P

EP = ("ep_0", "ep_1", "ep_2")
CHIPS = ("ep_0", "ep_1")
epsilon = 1e-06
CAP = 3


def eye(n):
    return lax.broadcasted_iota(jnp.int32, (n, n), 0) == lax.broadcasted_iota(jnp.int32, (n, n), 1)


def to_col(row, diag):
    return jnp.sum(jnp.where(diag, row, 0.0), axis=1, keepdims=True)


def to_row(col, diag):
    return jnp.sum(jnp.where(diag, col, 0.0), axis=0, keepdims=True)


def role(core, y):
    parity = jnp.where(core == 0, y // 2, (y + y // 2) % 2)
    half = jnp.where(core == 0, y % 2, y // 2)
    return parity, half


def partner(core, y, tp):
    return y ^ 1 if core == 0 else tp - 1 - y


def neighbour(core, y, tp):
    return partner(1 - core, y, tp)


def weight_moves(tp):
    edges = []
    for c in range(2):
        for y in range(tp):
            parity = y // 2 if c == 0 else (y + y // 2) % 2
            for n, s in enumerate((y, neighbour(c, y, tp))):
                if (parity, s) != (c, y):
                    edges.append(((parity, s), (c, y), n))
    color = {}

    def fits(i, r):
        return all(
            color[j] != r or (edges[j][0] != edges[i][0] and edges[j][1] != edges[i][1])
            for j in color
            if j != i
        )

    def place(i):
        if i == len(edges):
            return True
        for r in (1, 2):
            if fits(i, r):
                color[i] = r
                if place(i + 1):
                    return True
                del color[i]
        return False

    assert place(0)
    rounds = [[], []]
    comes = {(c, y): [0, 0] for c in range(2) for y in range(tp)}
    for i, (source, target, n) in enumerate(edges):
        rounds[color[i] - 1].append((source[0] * tp + source[1], target[0] * tp + target[1]))
        comes[target][n] = color[i]
    return rounds, comes


def spread(pieces_ref, scratch_ref):
    scratch_ref[...] = pieces_ref[...].astype(jnp.float32)
    return [chunk(scratch_ref, k)[...].astype(jnp.bfloat16) for k in range(CHUNKS)]


def chunk(scratch_ref, k):
    return scratch_ref.at[pl.ds(k, scratch_ref.shape[0] // CHUNKS, stride=CHUNKS), :]


def gathered(scratch_ref, out_ref):
    out_ref[...] = scratch_ref[...].astype(jnp.bfloat16)


def seat(chip, chips):
    place = chip + float(chips - FIRST % chips)
    return jnp.where(place < chips, place, place - chips)


def pre_kernel(
    tok_hbm,
    gain_hbm,
    ids_hbm,
    weight_hbm,
    post_hbm,
    gate_hbm,
    up_hbm,
    out_ref,
    place_ref,
    weight_ref,
    post_ref,
    both_ref,
    scratch_ref,
    tok_ref,
    gain_ref,
    ids_ref,
    stage_ref,
    sems,
    out_sems,
):
    rows, width = tok_ref.shape
    half = CHUNKS * 128
    slots = out_ref.shape[0] // CHUNKS
    chips = slots // CAP
    block = rows // PARTS
    pieces = [(ids_hbm, ids_ref)]
    for i in range(PARTS):
        span = pl.ds(i * block, block)
        pieces.append((tok_hbm.at[span, :], tok_ref.at[span, :]))
    pieces += [(gain_hbm, gain_ref), (weight_hbm, weight_ref), (post_hbm, post_ref)]
    pieces += [(gate_hbm, both_ref.at[0]), (up_hbm, both_ref.at[1])]
    copies = [pltpu.make_async_copy(a, b, sems.at[i]) for i, (a, b) in enumerate(pieces)]
    for copy in copies:
        copy.start()
    parity, side = role(lax.axis_index("ep_2"), lax.axis_index("tp"))
    parity = parity.astype(jnp.float32)
    start = pl.multiple_of(side * half, half)
    diag = eye(rows)
    lower = lax.broadcasted_iota(jnp.int32, (rows, rows), 0) < lax.broadcasted_iota(
        jnp.int32, (rows, rows), 1
    )
    copies[0].wait()
    ids = ids_ref[...].astype(jnp.float32)
    row0, row1 = ids[0:1, :], ids[1:2, :]
    col0, col1 = to_col(row0, diag), to_col(row1, diag)
    slot0 = jnp.sum(jnp.where((col0 == row0) & lower, 1.0, 0.0), axis=0, keepdims=True)
    slot1 = jnp.sum(jnp.where(col0 == row1, 1.0, 0.0), axis=0, keepdims=True) + jnp.sum(
        jnp.where((col1 == row1) & lower, 1.0, 0.0), axis=0, keepdims=True
    )
    chip0, chip1 = jnp.floor(row0 * 0.5), jnp.floor(row1 * 0.5)
    par0, par1 = row0 - 2.0 * chip0, row1 - 2.0 * chip1
    at0, at1 = CAP * seat(chip0, chips) + slot0, CAP * seat(chip1, chips) + slot1
    place_ref[0:1, :] = par0 * slots + at0
    place_ref[1:2, :] = par1 * slots + at1
    here0 = jnp.where(par0 == parity, at0, -1.0)
    here1 = jnp.where(par1 == parity, at1, -1.0)
    slot = lax.broadcasted_iota(jnp.int32, (slots, rows), 0).astype(jnp.float32)
    pick = jnp.where((slot == here0) | (slot == here1), 1.0, 0.0).astype(jnp.bfloat16)
    copies[PARTS + 1].wait()
    gain = gain_ref[:, pl.ds(start, half)]
    normed = []
    for i in range(PARTS):
        span = pl.ds(i * block, block)
        copies[1 + i].wait()
        values = tok_ref[span, :].astype(jnp.float32)
        scale = lax.rsqrt(jnp.mean(values * values, axis=1, keepdims=True) + epsilon)
        part = tok_ref[span, pl.ds(start, half)].astype(jnp.float32)
        normed.append((part * scale * gain).astype(jnp.bfloat16))
    normed = jnp.concatenate(normed, axis=0)
    outs = []
    share = slots // OUTS
    for i in range(OUTS):
        sent = jnp.dot(
            pick[i * share : (i + 1) * share], normed, preferred_element_type=jnp.float32
        )
        span = pl.ds(i * share * CHUNKS, share * CHUNKS)
        part_ref = scratch_ref.at[span, :]
        for k in range(CHUNKS):
            chunk(part_ref, k)[...] = sent[:, k * 128 : (k + 1) * 128]
        stage_ref[span, :] = part_ref[...].astype(jnp.bfloat16)
        outs.append(
            pltpu.make_async_copy(stage_ref.at[span, :], out_ref.at[span, :], out_sems.at[i])
        )
        outs[-1].start()
    for copy in copies[PARTS + 2 :] + outs:
        copy.wait()


def up_sums(pieces_ref, other, scratch_ref, weights, finish):
    half = CHUNKS * 128
    core, y = lax.axis_index("ep_2"), lax.axis_index("tp")
    side = role(core, y)[1]
    start = pl.multiple_of((1 - side if other else side) * half, half)
    rows = jnp.concatenate(spread(pieces_ref, scratch_ref), axis=1)

    def work(first, second):
        chosen = [(weights[r], i) for i in range(2) for r in (first, second)]
        columns = jnp.concatenate([w[i, pl.ds(start, half), :] for w, i in chosen], axis=1)
        finish(jnp.dot(rows, columns, preferred_element_type=jnp.float32))

    cases = {}
    for (c, t), comes in weight_moves(lax.axis_size("tp"))[1].items():
        cases.setdefault(tuple(comes), []).append((core == c) & (y == t))
    for comes, devices in sorted(cases.items()):
        here = devices[0]
        for device in devices[1:]:
            here = here | device
        pl.when(here)(lambda comes=comes: work(*comes))


def first_kernel(pieces_ref, w0, w1, w2, sums_ref, scratch_ref):
    def finish(sums):
        sums_ref[...] = sums

    up_sums(pieces_ref, False, scratch_ref, (w0, w1, w2), finish)


def hidden_kernel(pieces_ref, sums_ref, w0, w1, w2, out_ref, scratch_ref):
    def finish(sums):
        sums = sums_ref[...] + sums
        cols = out_ref.shape[2]
        gate, up = sums[:, :cols], sums[:, cols:]
        hidden = (gate / (1.0 + jnp.exp(-gate)) * up).astype(jnp.bfloat16)
        for i in range(out_ref.shape[0]):
            out_ref[i] = hidden

    up_sums(pieces_ref, True, scratch_ref, (w0, w1, w2), finish)


def down_kernel(hid_ref, mine_ref, other_ref, out_ref, scratch_ref):
    core = lax.axis_index("ep_2")
    slices = hid_ref.shape[0]
    wide = hid_ref.shape[2] // 2
    cols = mine_ref.shape[1]
    per = CHUNKS // 2

    def work(c, weights):
        for b, w in enumerate(weights):
            total = None
            for y in range(slices):
                if (y // 2 if c == 0 else (y + y // 2) % 2) != b:
                    continue
                for n, s in enumerate((y, neighbour(c, y, slices))):
                    add = jnp.dot(
                        hid_ref[y, :, n * wide : (n + 1) * wide],
                        w[s * wide : (s + 1) * wide, :],
                        preferred_element_type=jnp.float32,
                    )
                    total = add if total is None else total + add
            for k in range(per):
                chunk(scratch_ref, b * per + k)[...] = total[:, k * 128 : (k + 1) * 128]

    @pl.when(core == 0)
    def _():
        work(0, (mine_ref, other_ref))

    @pl.when(core == 1)
    def _():
        work(1, (other_ref, mine_ref))

    gathered(scratch_ref, out_ref)


def mix_kernel(back_ref, place_ref, weight_ref, mixed_ref, squares_ref, scratch_ref):
    slots = back_ref.shape[0] // CHUNKS
    rows, cols = mixed_ref.shape
    diag = eye(rows)
    lane = lax.broadcasted_iota(jnp.int32, (rows, slots), 1).astype(jnp.float32)
    pieces = spread(back_ref, scratch_ref)
    per = CHUNKS // 2
    back = [jnp.concatenate(pieces[b * per : (b + 1) * per], axis=1) for b in range(2)]
    mixed = None
    for k in range(2):
        place = to_col(place_ref[k : k + 1, :], diag)
        weight = to_col(weight_ref[k : k + 1, :], diag)
        picked = None
        for b in range(2):
            pick = jnp.where(lane + float(b * slots) == place, 1.0, 0.0).astype(jnp.bfloat16)
            add = jnp.dot(pick, back[b], preferred_element_type=jnp.float32)
            picked = add if picked is None else picked + add
        mixed = picked * weight if mixed is None else mixed + picked * weight
    mixed_ref[...] = mixed
    squares = to_row(jnp.sum(mixed * mixed, axis=1, keepdims=True), diag)
    squares_ref[...] = jnp.broadcast_to(squares[None], squares_ref.shape)


def norm_kernel(width, mixed_ref, squares_ref, gain_ref, out_ref):
    squares = jnp.sum(squares_ref[...], axis=0)[0:1, :]
    total = to_col(squares, eye(squares.shape[1]))
    scale = lax.rsqrt(total / width + epsilon)
    out_ref[...] = (mixed_ref[...] * scale * gain_ref[...]).astype(jnp.bfloat16)


CHUNKS = 8
PARTS = 2
OUTS = 4
FIRST = 40
WHOLE = pl.BlockSpec(memory_space=pltpu.VMEM)


def call(kernel, name, outs, *args, scratch=None):
    args = [pltpu.with_memory_space_constraint(a, pltpu.VMEM) for a in args]
    return pl.pallas_call(
        kernel,
        name=name,
        out_shape=outs,
        in_specs=[WHOLE] * len(args),
        out_specs=jax.tree.map(lambda _: WHOLE, outs, is_leaf=lambda o: hasattr(o, "dtype")),
        compiler_params=pltpu.CompilerParams(vmem_limit_bytes=16 << 20),
        scratch_shapes=[] if scratch is None else [pltpu.VMEM(scratch, jnp.float32)],
    )(*args)


def near(dims, dtype):
    return pltpu.VMEM(dims, dtype)


def per_device(tokens, pre_gain, post_gain, expert_ids, route_weights, w_gate, w_up, w_down):
    tok_rows, width = tokens.shape
    chips = lax.axis_size(CHIPS)
    tp = lax.axis_size("tp")
    slots = chips * CAP
    gate, up, down = w_gate[0], w_up[0], w_down[0]
    ff = gate.shape[1]
    cols = down.shape[1]
    flat = (slots * CHUNKS, 128)

    far = pl.BlockSpec(memory_space=pl.ANY)
    inputs = (
        tokens,
        pre_gain[None, :],
        expert_ids.T,
        route_weights.T,
        post_gain[None, :],
        gate,
        up,
    )
    buffer, place, mixing, post, both = pl.pallas_call(
        pre_kernel,
        name="pre",
        out_shape=(
            jax.ShapeDtypeStruct(flat, jnp.bfloat16),
            near((2, tok_rows), jnp.float32),
            near((2, tok_rows), jnp.float32),
            near((1, cols), jnp.float32),
            near((2, *gate.shape), gate.dtype),
        ),
        in_specs=[far] * len(inputs),
        out_specs=(far,) + (WHOLE,) * 4,
        compiler_params=pltpu.CompilerParams(vmem_limit_bytes=16 << 20),
        scratch_shapes=[
            pltpu.VMEM(flat, jnp.float32),
            pltpu.VMEM(tokens.shape, tokens.dtype),
            pltpu.VMEM(inputs[1].shape, jnp.float32),
            pltpu.VMEM(inputs[2].shape, jnp.int32),
            pltpu.VMEM(flat, jnp.bfloat16),
            pltpu.SemaphoreType.DMA((PARTS + 6,)),
            pltpu.SemaphoreType.DMA((OUTS,)),
        ],
    )(*[pltpu.with_memory_space_constraint(a, pltpu.HBM) for a in inputs])

    def exchange(rows):
        pieces = rows.reshape(chips, CAP * CHUNKS, 128)
        groups = [[(p + FIRST) % chips * 2 + c for p in range(chips)] for c in range(2)]
        return lax.all_to_all(
            pieces, EP, 0, 0, tiled=True, axis_index_groups=groups
        ).reshape(flat)

    with jax.named_scope("dispatch"):
        arrived = exchange(buffer)

    first, second = weight_moves(tp)[0]
    with jax.named_scope("weights"):
        moved = [lax.ppermute(both, ("ep_2", "tp"), moves) for moves in (first, second)]
        down_other = lax.ppermute(down, "ep_2", [(0, 1), (1, 0)])

    arrived, down_other = lax.optimization_barrier((arrived, down_other))
    with jax.named_scope("pair"):
        swaps = [(c * tp + t, c * tp + partner(c, t, tp)) for c in range(2) for t in range(tp)]
        theirs = lax.ppermute(arrived, ("ep_2", "tp"), swaps)
    weights = (both, *moved)
    sums = call(
        first_kernel, "first", near((slots, 4 * ff), jnp.float32), arrived, *weights, scratch=flat
    )
    hidden = call(
        hidden_kernel,
        "hidden",
        near((tp, slots, 2 * ff), jnp.bfloat16),
        theirs,
        sums,
        *weights,
        scratch=flat,
    )
    with jax.named_scope("gather"):
        hidden = lax.all_to_all(hidden, "tp", 0, 0, tiled=True)
    results = call(
        down_kernel, "down", near(flat, jnp.bfloat16), hidden, down, down_other, scratch=flat
    )
    with jax.named_scope("back"):
        returned = exchange(results)
    mixed, squares = call(
        mix_kernel,
        "mix",
        (near((tok_rows, cols), jnp.float32), near((tp, 1, tok_rows), jnp.float32)),
        returned,
        place,
        mixing,
        scratch=flat,
    )
    with jax.named_scope("squares"):
        squares = lax.all_to_all(squares, "tp", 0, 0, tiled=True, axis_index_groups=[[2, 3, 0, 1]])
    return call(
        lambda *refs: norm_kernel(width, *refs),
        "norm",
        jax.ShapeDtypeStruct((tok_rows, cols), jnp.bfloat16),
        mixed,
        squares,
        post,
    )


def solution(mesh):
    torus = Mesh(mesh.devices.reshape(16, 4, 2, mesh.shape["tp"]), ("ep_0", "ep_1", "ep_2", "tp"))
    in_specs = (
        P(EP, None),
        P(),
        P("tp"),
        P(EP, None),
        P(EP, None),
        P(EP, None, "tp"),
        P(EP, None, "tp"),
        P(EP, None, "tp"),
    )
    return jax.shard_map(
        per_device, mesh=torus, in_specs=in_specs, out_specs=P(EP, "tp"), check_vma=False
    )
```

```python
import jax
import jax.numpy as jnp
from jax import lax
from jax.experimental import pallas as pl
from jax.experimental.pallas import tpu as pltpu
from jax.sharding import Mesh
from jax.sharding import PartitionSpec as P

EP = ("ep_0", "ep_1", "ep_2")
CHIPS = ("ep_0", "ep_1")
epsilon = 1e-06
CAP = 3


def eye(n):
    return lax.broadcasted_iota(jnp.int32, (n, n), 0) == lax.broadcasted_iota(jnp.int32, (n, n), 1)


def to_col(row, diag):
    return jnp.sum(jnp.where(diag, row, 0.0), axis=1, keepdims=True)


def to_row(col, diag):
    return jnp.sum(jnp.where(diag, col, 0.0), axis=0, keepdims=True)


def role(core, y):
    parity = jnp.where(core == 0, y // 2, (y + y // 2) % 2)
    half = jnp.where(core == 0, y % 2, y // 2)
    return parity, half


def partner(core, y, tp):
    return y ^ 1 if core == 0 else tp - 1 - y


def neighbour(core, y, tp):
    return partner(1 - core, y, tp)


def weight_moves(tp):
    edges = []
    for c in range(2):
        for y in range(tp):
            parity = y // 2 if c == 0 else (y + y // 2) % 2
            for n, s in enumerate((y, neighbour(c, y, tp))):
                if (parity, s) != (c, y):
                    edges.append(((parity, s), (c, y), n))
    color = {}

    def fits(i, r):
        return all(
            color[j] != r or (edges[j][0] != edges[i][0] and edges[j][1] != edges[i][1])
            for j in color
            if j != i
        )

    def place(i):
        if i == len(edges):
            return True
        for r in (1, 2):
            if fits(i, r):
                color[i] = r
                if place(i + 1):
                    return True
                del color[i]
        return False

    assert place(0)
    rounds = [[], []]
    comes = {(c, y): [0, 0] for c in range(2) for y in range(tp)}
    for i, (source, target, n) in enumerate(edges):
        rounds[color[i] - 1].append((source[0] * tp + source[1], target[0] * tp + target[1]))
        comes[target][n] = color[i]
    return rounds, comes


def spread(pieces_ref, scratch_ref):
    scratch_ref[...] = pieces_ref[...].astype(jnp.float32)
    return [chunk(scratch_ref, k)[...].astype(jnp.bfloat16) for k in range(CHUNKS)]


def chunk(scratch_ref, k):
    return scratch_ref.at[pl.ds(k, scratch_ref.shape[0] // CHUNKS, stride=CHUNKS), :]


def gathered(scratch_ref, out_ref):
    out_ref[...] = scratch_ref[...].astype(jnp.bfloat16)


def seat(chip, chips):
    place = chip + float(chips - FIRST % chips)
    return jnp.where(place < chips, place, place - chips)


def pre_kernel(
    tok_hbm,
    gain_hbm,
    ids_hbm,
    weight_hbm,
    post_hbm,
    gate_hbm,
    up_hbm,
    out_ref,
    place_ref,
    weight_ref,
    post_ref,
    both_ref,
    scratch_ref,
    tok_ref,
    gain_ref,
    ids_ref,
    stage_ref,
    sems,
    out_sems,
):
    rows, width = tok_ref.shape
    half = CHUNKS * 128
    slots = out_ref.shape[0] // CHUNKS
    chips = slots // CAP
    block = rows // PARTS
    pieces = [(ids_hbm, ids_ref)]
    for i in range(PARTS):
        span = pl.ds(i * block, block)
        pieces.append((tok_hbm.at[span, :], tok_ref.at[span, :]))
    pieces += [(gain_hbm, gain_ref), (weight_hbm, weight_ref), (post_hbm, post_ref)]
    pieces += [(gate_hbm, both_ref.at[0]), (up_hbm, both_ref.at[1])]
    copies = [pltpu.make_async_copy(a, b, sems.at[i]) for i, (a, b) in enumerate(pieces)]
    for copy in copies:
        copy.start()
    parity, side = role(lax.axis_index("ep_2"), lax.axis_index("tp"))
    parity = parity.astype(jnp.float32)
    start = pl.multiple_of(side * half, half)
    diag = eye(rows)
    lower = lax.broadcasted_iota(jnp.int32, (rows, rows), 0) < lax.broadcasted_iota(
        jnp.int32, (rows, rows), 1
    )
    copies[0].wait()
    ids = ids_ref[...].astype(jnp.float32)
    row0, row1 = ids[0:1, :], ids[1:2, :]
    col0, col1 = to_col(row0, diag), to_col(row1, diag)
    slot0 = jnp.sum(jnp.where((col0 == row0) & lower, 1.0, 0.0), axis=0, keepdims=True)
    slot1 = jnp.sum(jnp.where(col0 == row1, 1.0, 0.0), axis=0, keepdims=True) + jnp.sum(
        jnp.where((col1 == row1) & lower, 1.0, 0.0), axis=0, keepdims=True
    )
    chip0, chip1 = jnp.floor(row0 * 0.5), jnp.floor(row1 * 0.5)
    par0, par1 = row0 - 2.0 * chip0, row1 - 2.0 * chip1
    at0, at1 = CAP * seat(chip0, chips) + slot0, CAP * seat(chip1, chips) + slot1
    place_ref[0:1, :] = par0 * slots + at0
    place_ref[1:2, :] = par1 * slots + at1
    here0 = jnp.where(par0 == parity, at0, -1.0)
    here1 = jnp.where(par1 == parity, at1, -1.0)
    slot = lax.broadcasted_iota(jnp.int32, (slots, rows), 0).astype(jnp.float32)
    pick = jnp.where((slot == here0) | (slot == here1), 1.0, 0.0).astype(jnp.bfloat16)
    copies[PARTS + 1].wait()
    gain = gain_ref[:, pl.ds(start, half)]
    normed = []
    for i in range(PARTS):
        span = pl.ds(i * block, block)
        copies[1 + i].wait()
        values = tok_ref[span, :].astype(jnp.float32)
        scale = lax.rsqrt(jnp.mean(values * values, axis=1, keepdims=True) + epsilon)
        part = tok_ref[span, pl.ds(start, half)].astype(jnp.float32)
        normed.append((part * scale * gain).astype(jnp.bfloat16))
    normed = jnp.concatenate(normed, axis=0)
    outs = []
    share = slots // OUTS
    for i in range(OUTS):
        sent = jnp.dot(
            pick[i * share : (i + 1) * share], normed, preferred_element_type=jnp.float32
        )
        span = pl.ds(i * share * CHUNKS, share * CHUNKS)
        part_ref = scratch_ref.at[span, :]
        for k in range(CHUNKS):
            chunk(part_ref, k)[...] = sent[:, k * 128 : (k + 1) * 128]
        stage_ref[span, :] = part_ref[...].astype(jnp.bfloat16)
        outs.append(
            pltpu.make_async_copy(stage_ref.at[span, :], out_ref.at[span, :], out_sems.at[i])
        )
        outs[-1].start()
    for copy in copies[PARTS + 2 :] + outs:
        copy.wait()


def up_sums(pieces_ref, other, scratch_ref, weights, finish):
    half = CHUNKS * 128
    core, y = lax.axis_index("ep_2"), lax.axis_index("tp")
    side = role(core, y)[1]
    start = pl.multiple_of((1 - side if other else side) * half, half)
    rows = jnp.concatenate(spread(pieces_ref, scratch_ref), axis=1)

    def work(first, second):
        chosen = [(weights[r], i) for i in range(2) for r in (first, second)]
        columns = jnp.concatenate([w[i, pl.ds(start, half), :] for w, i in chosen], axis=1)
        finish(jnp.dot(rows, columns, preferred_element_type=jnp.float32))

    cases = {}
    for (c, t), comes in weight_moves(lax.axis_size("tp"))[1].items():
        cases.setdefault(tuple(comes), []).append((core == c) & (y == t))
    for comes, devices in sorted(cases.items()):
        here = devices[0]
        for device in devices[1:]:
            here = here | device
        pl.when(here)(lambda comes=comes: work(*comes))


def first_kernel(pieces_ref, w0, w1, w2, sums_ref, scratch_ref):
    def finish(sums):
        sums_ref[...] = sums

    up_sums(pieces_ref, False, scratch_ref, (w0, w1, w2), finish)


def hidden_kernel(pieces_ref, sums_ref, w0, w1, w2, out_ref, scratch_ref):
    def finish(sums):
        sums = sums_ref[...] + sums
        cols = out_ref.shape[2]
        gate, up = sums[:, :cols], sums[:, cols:]
        hidden = (gate / (1.0 + jnp.exp(-gate)) * up).astype(jnp.bfloat16)
        for i in range(out_ref.shape[0]):
            out_ref[i] = hidden

    up_sums(pieces_ref, True, scratch_ref, (w0, w1, w2), finish)


def down_kernel(hid_ref, mine_ref, other_ref, out_ref, scratch_ref):
    core = lax.axis_index("ep_2")
    slices = hid_ref.shape[0]
    wide = hid_ref.shape[2] // 2
    cols = mine_ref.shape[1]
    per = CHUNKS // 2

    def work(c, weights):
        for b, w in enumerate(weights):
            total = None
            for y in range(slices):
                if (y // 2 if c == 0 else (y + y // 2) % 2) != b:
                    continue
                for n, s in enumerate((y, neighbour(c, y, slices))):
                    add = jnp.dot(
                        hid_ref[y, :, n * wide : (n + 1) * wide],
                        w[s * wide : (s + 1) * wide, :],
                        preferred_element_type=jnp.float32,
                    )
                    total = add if total is None else total + add
            for k in range(per):
                chunk(scratch_ref, b * per + k)[...] = total[:, k * 128 : (k + 1) * 128]

    @pl.when(core == 0)
    def _():
        work(0, (mine_ref, other_ref))

    @pl.when(core == 1)
    def _():
        work(1, (other_ref, mine_ref))

    gathered(scratch_ref, out_ref)


def mix_kernel(back_ref, place_ref, weight_ref, mixed_ref, squares_ref, scratch_ref):
    slots = back_ref.shape[0] // CHUNKS
    rows, cols = mixed_ref.shape
    diag = eye(rows)
    lane = lax.broadcasted_iota(jnp.int32, (rows, slots), 1).astype(jnp.float32)
    pieces = spread(back_ref, scratch_ref)
    per = CHUNKS // 2
    back = [jnp.concatenate(pieces[b * per : (b + 1) * per], axis=1) for b in range(2)]
    mixed = None
    for k in range(2):
        place = to_col(place_ref[k : k + 1, :], diag)
        weight = to_col(weight_ref[k : k + 1, :], diag)
        picked = None
        for b in range(2):
            pick = jnp.where(lane + float(b * slots) == place, 1.0, 0.0).astype(jnp.bfloat16)
            add = jnp.dot(pick, back[b], preferred_element_type=jnp.float32)
            picked = add if picked is None else picked + add
        mixed = picked * weight if mixed is None else mixed + picked * weight
    mixed_ref[...] = mixed
    squares = to_row(jnp.sum(mixed * mixed, axis=1, keepdims=True), diag)
    squares_ref[...] = jnp.broadcast_to(squares[None], squares_ref.shape)


def norm_kernel(width, mixed_ref, squares_ref, gain_ref, out_ref):
    squares = jnp.sum(squares_ref[...], axis=0)[0:1, :]
    total = to_col(squares, eye(squares.shape[1]))
    scale = lax.rsqrt(total / width + epsilon)
    out_ref[...] = (mixed_ref[...] * scale * gain_ref[...]).astype(jnp.bfloat16)


CHUNKS = 8
PARTS = 2
OUTS = 4
FIRST = 44
WHOLE = pl.BlockSpec(memory_space=pltpu.VMEM)


def call(kernel, name, outs, *args, scratch=None):
    args = [pltpu.with_memory_space_constraint(a, pltpu.VMEM) for a in args]
    return pl.pallas_call(
        kernel,
        name=name,
        out_shape=outs,
        in_specs=[WHOLE] * len(args),
        out_specs=jax.tree.map(lambda _: WHOLE, outs, is_leaf=lambda o: hasattr(o, "dtype")),
        compiler_params=pltpu.CompilerParams(vmem_limit_bytes=16 << 20),
        scratch_shapes=[] if scratch is None else [pltpu.VMEM(scratch, jnp.float32)],
    )(*args)


def near(dims, dtype):
    return pltpu.VMEM(dims, dtype)


def per_device(tokens, pre_gain, post_gain, expert_ids, route_weights, w_gate, w_up, w_down):
    tok_rows, width = tokens.shape
    chips = lax.axis_size(CHIPS)
    tp = lax.axis_size("tp")
    slots = chips * CAP
    gate, up, down = w_gate[0], w_up[0], w_down[0]
    ff = gate.shape[1]
    cols = down.shape[1]
    flat = (slots * CHUNKS, 128)

    far = pl.BlockSpec(memory_space=pl.ANY)
    inputs = (
        tokens,
        pre_gain[None, :],
        expert_ids.T,
        route_weights.T,
        post_gain[None, :],
        gate,
        up,
    )
    buffer, place, mixing, post, both = pl.pallas_call(
        pre_kernel,
        name="pre",
        out_shape=(
            jax.ShapeDtypeStruct(flat, jnp.bfloat16),
            near((2, tok_rows), jnp.float32),
            near((2, tok_rows), jnp.float32),
            near((1, cols), jnp.float32),
            near((2, *gate.shape), gate.dtype),
        ),
        in_specs=[far] * len(inputs),
        out_specs=(far,) + (WHOLE,) * 4,
        compiler_params=pltpu.CompilerParams(vmem_limit_bytes=16 << 20),
        scratch_shapes=[
            pltpu.VMEM(flat, jnp.float32),
            pltpu.VMEM(tokens.shape, tokens.dtype),
            pltpu.VMEM(inputs[1].shape, jnp.float32),
            pltpu.VMEM(inputs[2].shape, jnp.int32),
            pltpu.VMEM(flat, jnp.bfloat16),
            pltpu.SemaphoreType.DMA((PARTS + 6,)),
            pltpu.SemaphoreType.DMA((OUTS,)),
        ],
    )(*[pltpu.with_memory_space_constraint(a, pltpu.HBM) for a in inputs])

    def exchange(rows):
        pieces = rows.reshape(chips, CAP * CHUNKS, 128)
        groups = [[(p + FIRST) % chips * 2 + c for p in range(chips)] for c in range(2)]
        return lax.all_to_all(
            pieces, EP, 0, 0, tiled=True, axis_index_groups=groups
        ).reshape(flat)

    with jax.named_scope("dispatch"):
        arrived = exchange(buffer)

    first, second = weight_moves(tp)[0]
    with jax.named_scope("weights"):
        moved = [lax.ppermute(both, ("ep_2", "tp"), moves) for moves in (first, second)]
        down_other = lax.ppermute(down, "ep_2", [(0, 1), (1, 0)])

    arrived, down_other = lax.optimization_barrier((arrived, down_other))
    with jax.named_scope("pair"):
        swaps = [(c * tp + t, c * tp + partner(c, t, tp)) for c in range(2) for t in range(tp)]
        theirs = lax.ppermute(arrived, ("ep_2", "tp"), swaps)
    weights = (both, *moved)
    sums = call(
        first_kernel, "first", near((slots, 4 * ff), jnp.float32), arrived, *weights, scratch=flat
    )
    hidden = call(
        hidden_kernel,
        "hidden",
        near((tp, slots, 2 * ff), jnp.bfloat16),
        theirs,
        sums,
        *weights,
        scratch=flat,
    )
    with jax.named_scope("gather"):
        hidden = lax.all_to_all(hidden, "tp", 0, 0, tiled=True)
    results = call(
        down_kernel, "down", near(flat, jnp.bfloat16), hidden, down, down_other, scratch=flat
    )
    with jax.named_scope("back"):
        returned = exchange(results)
    mixed, squares = call(
        mix_kernel,
        "mix",
        (near((tok_rows, cols), jnp.float32), near((tp, 1, tok_rows), jnp.float32)),
        returned,
        place,
        mixing,
        scratch=flat,
    )
    with jax.named_scope("squares"):
        squares = lax.all_to_all(squares, "tp", 0, 0, tiled=True, axis_index_groups=[[2, 3, 0, 1]])
    return call(
        lambda *refs: norm_kernel(width, *refs),
        "norm",
        jax.ShapeDtypeStruct((tok_rows, cols), jnp.bfloat16),
        mixed,
        squares,
        post,
    )


def solution(mesh):
    torus = Mesh(mesh.devices.reshape(16, 4, 2, mesh.shape["tp"]), ("ep_0", "ep_1", "ep_2", "tp"))
    in_specs = (
        P(EP, None),
        P(),
        P("tp"),
        P(EP, None),
        P(EP, None),
        P(EP, None, "tp"),
        P(EP, None, "tp"),
        P(EP, None, "tp"),
    )
    return jax.shard_map(
        per_device, mesh=torus, in_specs=in_specs, out_specs=P(EP, "tp"), check_vma=False
    )
```
